512 devices in a mesh: ep: 128 (over z, x, core), tp: 4 (over y).
Axes of the slice: x: 4, y: 4, z: 16, core: 2. Of those that a mesh axis runs over, the one named last changes fastest.
Arguments:
- tokens: bfloat16 [6144, 1024], P('ep'), may hold values from -6 to 6
- head_state: float32 [6144, 8, 64, 64], P('ep', 'tp'), may hold values from -6 to 6
- recept_weight: bfloat16 [1024, 512], P(None, 'tp'), may hold values from -0.1875 to 0.1875
- key_weight: bfloat16 [1024, 512], P(None, 'tp'), may hold values from -0.1875 to 0.1875
- value_weight: bfloat16 [1024, 512], P(None, 'tp'), may hold values from -0.1875 to 0.1875
- decay_down_factor: bfloat16 [1024, 64], replicated, may hold values from -0.1875 to 0.1875
- decay_up_factor: bfloat16 [64, 512], P(None, 'tp'), may hold values from -0.75 to 0.75
- decay_base: float32 [512], P('tp'), may hold values from -5 to 3
- rate_down_factor: bfloat16 [1024, 64], replicated, may hold values from -0.1875 to 0.1875
- rate_up_factor: bfloat16 [64, 512], P(None, 'tp'), may hold values from -0.75 to 0.75
- rate_base: float32 [512], P('tp'), may hold values from -3 to 3
- head_gain: float32 [512], P('tp'), may hold values from 0.1 to 1.9
- out_weight: bfloat16 [512, 1024], P('tp'), may hold values from -0.25 to 0.25
- route_experts: int32 [6144, 4], P('ep'), may hold values from 0 to 127, all different within a row; in each aligned block of 48 rows (0 to 47, 48 to 95, ...) at most 3 rows name the same one
- route_weights: float32 [6144, 4], P('ep'), may hold values from 0.03 to 0.2
- expert_gate: bfloat16 [128, 1024, 1024], P('ep', None, 'tp'), may hold values from -1 to 1
- expert_up: bfloat16 [128, 1024, 1024], P('ep', None, 'tp'), may hold values from -1 to 1
- expert_down: bfloat16 [128, 1024, 1024], P('ep', 'tp'), may hold values from -0.1875 to 0.1875
Outputs:
- layer_out: bfloat16 [6144, 1024], P('ep', 'tp')
- new_state: float32 [6144, 8, 64, 64], P('ep', 'tp')
The draws below stay inside these ranges and needn't reach their ends.
Inputs may be any that keep to these rules, and one draw needn't show every extreme that they name: `route_experts`: each row names 4 different experts. In each aligned block of 48 rows no expert is named by more than 3 rows, a bound that some block reaches.
All inputs are finite; a program needn't handle non-finite values.
Results may differ from the reference program's by a relative error of at most 0.02.
Values may be sent and summed in bfloat16 or wider, within the bound.
A program may use at most 128 MiB of HBM per device.

```python
import math
import jax
import jax.numpy as jnp
import numpy as np
from jax import lax

MODEL_DIMENSION = 1024
ALL_HEADS_WIDTH = 512
HEAD_DIM = 64
HEADS = 8
LOW_RANK_WIDTH = 64
DE = 1024
TOP_K = 4
SEQ_DEV = 48
SEQS = 6144
EXPERTS = 128
CAP = 3
N_EP = 128
N_TP = 4


def column_scaled(key, stream):
    folded = jax.random.fold_in(key, stream)
    entries = jax.random.truncated_normal(jax.random.fold_in(folded, 1), -6.0, 6.0, (EXPERTS, MODEL_DIMENSION, DE), jnp.float32)
    column_scale = jnp.exp(jax.random.uniform(jax.random.fold_in(folded, 2), (EXPERTS, 1, DE), jnp.float32) * math.log(8.0))
    return jnp.clip(entries * column_scale / math.sqrt(MODEL_DIMENSION), -1.0, 1.0).astype(jnp.bfloat16)


def draw_expert_gate(key, part):
    return column_scaled(key, 11)


def draw_expert_up(key, part):
    return column_scaled(key, 23)


def block_levels(rng, shape, pieces, smallest, high):
    loudness, own = 1.0, jax.random.fold_in(rng, 6)
    for position, shards_of in pieces:
        heights = jnp.exp(jax.random.uniform(jax.random.fold_in(own, position), (shards_of,), jnp.float32, smallest / len(pieces), high / len(pieces)))
        loudness = loudness * jnp.repeat(heights, shape[position] // shards_of).reshape([-1 if axis == position else 1 for axis in range(len(shape))])
    return loudness


def shared_out(key, own, number, rows, count, top, bound, lean):
    sequence = jax.random.permutation(key, count)
    crowded, usual = load_shares(count, rows * top, bound, lean, True), load_shares(count, rows * top, bound, lean, False)
    places = jnp.arange(count)

    def named(sizes, offset_by):
        used = int((sizes > 0).sum())
        fixed = max(1, used // 4)
        moved = fixed + (places - fixed + offset_by * (used - fixed)) % max(1, count - fixed)
        return jnp.zeros((count,), jnp.int32).at[sequence[jnp.where(places < fixed, places, moved)]].set(jnp.asarray(sizes, jnp.int32))

    sizes = jnp.where(number % 4 == 0, named(crowded, number // 4), named(usual, number - number // 4 - 1))
    mixed = jax.random.permutation(jax.random.fold_in(own, 3), count)
    source_of, sink = mixed[0:count // 2 * 2:2], mixed[1:count // 2 * 2:2]
    slack = jnp.minimum(sizes[source_of] - 1, bound - sizes[sink]) // 2
    slack = jnp.where((source_of == sequence[0]) | (sink == sequence[0]) | (sizes[sink] == 0), 0, jnp.maximum(slack, 0))
    moved = jax.random.randint(jax.random.fold_in(own, 4), (count // 2,), 0, 1 << 20) % (slack + 1)
    sizes = sizes.at[source_of].add(-moved).at[sink].add(moved)
    labels = jnp.searchsorted(jnp.cumsum(sizes), jnp.arange(rows * top), side="right").astype(jnp.int32)
    grid = labels.reshape(top, rows).T
    grid = grid[jax.random.permutation(jax.random.fold_in(own, 1), rows)]
    offset_by = jax.random.randint(jax.random.fold_in(own, 2), (rows, 1), 0, top)
    return jnp.take_along_axis(grid, (jnp.arange(top)[None, :] + offset_by) % top, axis=1)


def load_shares(number_of, total, most, lean, full):
    weights = [(1 << 20) // math.isqrt(grade ** lean) + 1 for grade in range(1, number_of + 1)]
    largest = most if full else min(most, max(-(-total // number_of), total * weights[0] // sum(weights)))
    least = 1 if total - largest >= number_of - 1 else 0
    counts, rest = [largest] + [least] * (number_of - 1), total - largest - least * (number_of - 1)
    while rest > 0:
        movable = [i for i in range(1, number_of) if counts[i] < largest] or [i for i in range(1, number_of) if counts[i] < most]
        mass, budget = sum([weights[i] for i in movable]), rest
        for i in movable:
            addition = min(most - counts[i], max(1, budget * weights[i] // mass), rest)
            counts[i] = counts[i] + addition
            rest = rest - addition
    return np.array(counts)


def gaussian(own_key, dims, scale, bound, cuts=(), kind=jnp.bfloat16):
    result = jax.random.normal(own_key, dims, jnp.float32) * scale
    if len(cuts) > 0:
        result = block_levels(own_key, dims, cuts, -0.22, 0.18) * result
    return jnp.clip(result, min=-bound, max=bound).astype(kind)


def setup_inputs(seed: int = 0) -> dict:
    arg_keys = jax.random.split(jax.random.key(seed), 19)
    tokens = gaussian(arg_keys[0], (SEQS, MODEL_DIMENSION), 1.0, 6.0, ((0, 128),))
    head_state = gaussian(arg_keys[1], (SEQS, HEADS, HEAD_DIM, HEAD_DIM), 1.0, 6.0, ((0, 128), (1, 4)), jnp.float32)
    recept_weight = gaussian(arg_keys[2], (MODEL_DIMENSION, ALL_HEADS_WIDTH), MODEL_DIMENSION ** -0.5, 0.1875, ((1, 4),))
    key_weight = gaussian(arg_keys[3], (MODEL_DIMENSION, ALL_HEADS_WIDTH), MODEL_DIMENSION ** -0.5, 0.1875, ((1, 4),))
    value_weight = gaussian(arg_keys[4], (MODEL_DIMENSION, ALL_HEADS_WIDTH), MODEL_DIMENSION ** -0.5, 0.1875, ((1, 4),))
    decay_down_factor = gaussian(arg_keys[5], (MODEL_DIMENSION, LOW_RANK_WIDTH), MODEL_DIMENSION ** -0.5, 0.1875)
    decay_up_factor = gaussian(arg_keys[6], (LOW_RANK_WIDTH, ALL_HEADS_WIDTH), LOW_RANK_WIDTH ** -0.5, 0.75, ((1, 4),))
    decay_base = jnp.clip(-5.0 + 8.0 * jax.random.uniform(arg_keys[7], (ALL_HEADS_WIDTH,), jnp.float32) ** block_levels(arg_keys[7], (ALL_HEADS_WIDTH,), ((0, 4),), -0.2, 0.2), -5.0, 3.0)
    rate_down_factor = gaussian(arg_keys[8], (MODEL_DIMENSION, LOW_RANK_WIDTH), MODEL_DIMENSION ** -0.5, 0.1875)
    rate_up_factor = gaussian(arg_keys[9], (LOW_RANK_WIDTH, ALL_HEADS_WIDTH), LOW_RANK_WIDTH ** -0.5, 0.75, ((1, 4),))
    rate_base = jnp.clip(jax.random.uniform(arg_keys[10], (ALL_HEADS_WIDTH,), jnp.float32, -3.0, 3.0) * block_levels(arg_keys[10], (ALL_HEADS_WIDTH,), ((0, 4),), -0.4, 0.0), -3.0, 3.0)
    head_gain = jnp.clip(1.0 + 0.18 * jax.random.normal(arg_keys[11], (ALL_HEADS_WIDTH,), jnp.float32), 0.1, 1.9)
    out_weight = gaussian(arg_keys[12], (ALL_HEADS_WIDTH, MODEL_DIMENSION), ALL_HEADS_WIDTH ** -0.5, 0.25, ((0, 4),))
    route_experts_keys = jax.random.split(jax.random.fold_in(arg_keys[13], 1), SEQS // SEQ_DEV)
    route_experts_turns = jax.random.permutation(jax.random.fold_in(arg_keys[13], 3), SEQS // SEQ_DEV)
    route_experts = jax.vmap(lambda own, number: shared_out(jax.random.fold_in(arg_keys[13], 2), own, number, SEQ_DEV, EXPERTS, TOP_K, CAP, 2))(route_experts_keys, route_experts_turns).reshape((SEQS, TOP_K))
    route_weights = jnp.clip(jnp.exp(math.log(0.2) - 1.89712 * jax.random.uniform(arg_keys[14], (SEQS, TOP_K), jnp.float32) ** block_levels(arg_keys[14], (SEQS, TOP_K), ((0, 128),), -0.2, 0.2)), 0.03, 0.2)
    expert_gate = draw_expert_gate(jax.random.fold_in(arg_keys[18], 71), 0)
    expert_up = draw_expert_up(jax.random.fold_in(arg_keys[18], 71), 0)
    expert_down = gaussian(arg_keys[17], (EXPERTS, DE, MODEL_DIMENSION), DE ** -0.5, 0.1875, ((0, 128), (1, 4)))
    return dict(tokens=tokens, head_state=head_state, recept_weight=recept_weight, key_weight=key_weight, value_weight=value_weight, decay_down_factor=decay_down_factor, decay_up_factor=decay_up_factor, decay_base=decay_base, rate_down_factor=rate_down_factor, rate_up_factor=rate_up_factor, rate_base=rate_base, head_gain=head_gain, out_weight=out_weight, route_experts=route_experts, route_weights=route_weights, expert_gate=expert_gate, expert_up=expert_up, expert_down=expert_down)


NORM_EPS = 1e-05
GROUP_EPS = 0.00064
UNIT_EPS = 1e-06
CLAMP_LIMIT = 7.0
GLU_ALPHA = 1.702

def row_norm(values):
    return values * lax.rsqrt(lax.optimization_barrier(jnp.mean(values * values, axis=-1, keepdims=True)) + NORM_EPS)

def clamped_unit(gate_pre, up_pre):
    gated = jnp.minimum(gate_pre, CLAMP_LIMIT)
    linear = jnp.clip(up_pre, -CLAMP_LIMIT, CLAMP_LIMIT)
    return gated * jax.nn.sigmoid(GLU_ALPHA * gated) * (linear + 1.0)

def update_heads(head_state, recept, keys, values, decay_rate, rate_gate, head_gain):
    seq_count, head_count, head_size = head_state.shape[:3]

    def by_heads(operand):
        return operand.astype(jnp.float32).reshape(seq_count, head_count, head_size)
    recept_heads = by_heads(recept)
    key_heads = by_heads(keys)
    value_heads = by_heads(values)
    decay_heads = by_heads(decay_rate)
    rate_heads = by_heads(rate_gate)
    unit_key = key_heads * lax.rsqrt(lax.optimization_barrier(jnp.sum(key_heads * key_heads, axis=-1, keepdims=True)) + UNIT_EPS)
    highest = lax.Precision.HIGHEST
    state_unit = jnp.einsum('shvk,shk->shv', head_state, unit_key, precision=highest)
    new_state = head_state * decay_heads[:, :, None, :] - state_unit[..., None] * (unit_key * rate_heads)[:, :, None, :] + value_heads[..., None] * (key_heads * rate_heads)[:, :, None, :]
    head_out = jnp.einsum('shvk,shk->shv', new_state, recept_heads, precision=highest)
    centre = lax.optimization_barrier(jnp.mean(head_out, axis=-1, keepdims=True))
    spread = lax.optimization_barrier(jnp.mean(jnp.square(head_out - centre), axis=-1, keepdims=True))
    normed_heads = (head_out - centre) * lax.rsqrt(spread + GROUP_EPS)
    mixed = (normed_heads.reshape(seq_count, -1) * head_gain).astype(jnp.bfloat16)
    return (new_state, mixed)

def reference(tokens, head_state, recept_weight, key_weight, value_weight, decay_down_factor, decay_up_factor, decay_base, rate_down_factor, rate_up_factor, rate_base, head_gain, out_weight, route_experts, route_weights, expert_gate, expert_up, expert_down):
    tokens_float = tokens.astype(jnp.float32)
    normed = row_norm(tokens_float).astype(jnp.bfloat16)
    recept = jnp.dot(normed, recept_weight, preferred_element_type=jnp.float32).astype(jnp.bfloat16)
    keys = jnp.dot(normed, key_weight, preferred_element_type=jnp.float32).astype(jnp.bfloat16)
    values = jnp.dot(normed, value_weight, preferred_element_type=jnp.float32).astype(jnp.bfloat16)
    decay_low = jnp.tanh(jnp.dot(normed, decay_down_factor, preferred_element_type=jnp.float32)).astype(jnp.bfloat16)
    rate_low = jnp.dot(normed, rate_down_factor, preferred_element_type=jnp.float32).astype(jnp.bfloat16)
    decay_pre = decay_base + jnp.dot(decay_low, decay_up_factor, preferred_element_type=jnp.float32)
    decay_rate = jnp.exp(-jnp.exp(-jax.nn.softplus(-decay_pre) - 0.5))
    rate_gate = jax.nn.sigmoid(rate_base + jnp.dot(rate_low, rate_up_factor, preferred_element_type=jnp.float32))
    new_state, mixed = update_heads(head_state, recept, keys, values, decay_rate, rate_gate, head_gain)
    group_width = ALL_HEADS_WIDTH // N_TP
    partials = jnp.einsum('sgr,grd->gsd', mixed.reshape(SEQS, N_TP, group_width).astype(jnp.float32), out_weight.reshape(N_TP, group_width, MODEL_DIMENSION).astype(jnp.float32))
    partials = lax.optimization_barrier(partials.astype(jnp.bfloat16)).astype(jnp.float32)
    residual = (tokens_float + lax.optimization_barrier(jnp.sum(partials, axis=0))).astype(jnp.bfloat16)
    expert_input = row_norm(residual.astype(jnp.float32)).astype(jnp.bfloat16)
    grouped = route_experts.reshape(N_EP, SEQ_DEV * TOP_K)
    onehot = (grouped[:, :, None] == jnp.arange(EXPERTS, dtype=jnp.int32)[None, None, :]).astype(jnp.int32)
    earlier = jnp.cumsum(onehot, axis=1) - onehot
    slot_rank = lax.optimization_barrier(jnp.sum(earlier * onehot, axis=-1)).astype(jnp.int32)
    target = (grouped * CAP + slot_rank).astype(jnp.int32)
    repeated = jnp.repeat(expert_input.reshape(N_EP, SEQ_DEV, MODEL_DIMENSION), TOP_K, axis=1)
    sources = jnp.arange(N_EP, dtype=jnp.int32)[:, None]
    buffer = jnp.zeros((N_EP, EXPERTS * CAP, MODEL_DIMENSION), jnp.bfloat16).at[sources, target].set(repeated)
    per_expert = buffer.reshape(N_EP, EXPERTS, CAP, MODEL_DIMENSION).transpose(1, 0, 2, 3).reshape(EXPERTS, N_EP * CAP, MODEL_DIMENSION)
    hidden_group = DE // N_TP

    def one_expert(operands):
        slot_rows, gate_matrix, up_matrix, down_matrix = operands
        gate_pre = jnp.dot(slot_rows, gate_matrix, preferred_element_type=jnp.float32)
        up_pre = jnp.dot(slot_rows, up_matrix, preferred_element_type=jnp.float32)
        activated = clamped_unit(gate_pre, up_pre).astype(jnp.bfloat16)
        expert_parts = jnp.einsum('rgc,gcd->grd', activated.reshape(-1, N_TP, hidden_group).astype(jnp.float32), down_matrix.reshape(N_TP, hidden_group, MODEL_DIMENSION).astype(jnp.float32))
        expert_parts = lax.optimization_barrier(expert_parts.astype(jnp.bfloat16)).astype(jnp.float32)
        return lax.optimization_barrier(jnp.sum(expert_parts, axis=0)).astype(jnp.bfloat16)
    results = lax.map(one_expert, (per_expert, expert_gate, expert_up, expert_down))
    returned = results.reshape(EXPERTS, N_EP, CAP, MODEL_DIMENSION).transpose(1, 0, 2, 3).reshape(N_EP, EXPERTS * CAP, MODEL_DIMENSION)
    picked = jnp.take_along_axis(returned, target[:, :, None], axis=1)
    picked = picked.reshape(SEQS, TOP_K, MODEL_DIMENSION).astype(jnp.float32)
    mixture = lax.optimization_barrier(jnp.sum(route_weights[:, :, None] * picked, axis=1))
    layer_out = (residual.astype(jnp.float32) + mixture).astype(jnp.bfloat16)
    return (layer_out, new_state)
```

```python
import functools

import jax
import jax.numpy as jnp
from jax import lax
from jax.experimental import pallas as pl
from jax.experimental.pallas import tpu as pltpu
from jax.sharding import PartitionSpec as P

NORM_EPS = 1e-05
GROUP_EPS = 0.00064
UNIT_EPS = 1e-06
CLAMP_LIMIT = 7.0
GLU_ALPHA = 1.702
PLANE = 8
SLOTS = 3
LANES = 128
GROUP = 4
MESH = pl.DeviceIdType.MESH
F32, BF16, I32 = jnp.float32, jnp.bfloat16, jnp.int32


def plane_offset(j):
    half = (j + 1) // 2
    return half if j % 2 else -half


def row_norm(values):
    return values * lax.rsqrt(jnp.mean(values * values, axis=-1, keepdims=True) + NORM_EPS)


def update_heads(head_state, recept, keys, values, decay_rate, rate_gate, head_gain):
    seq_count, head_count, head_size = head_state.shape[:3]

    def by_heads(operand):
        return operand.astype(jnp.float32).reshape(seq_count, head_count, head_size)

    recept_heads = by_heads(recept)
    key_heads = by_heads(keys)
    value_heads = by_heads(values)
    decay_heads = by_heads(decay_rate)
    rate_heads = by_heads(rate_gate)
    unit_key = key_heads * lax.rsqrt(
        jnp.sum(key_heads * key_heads, axis=-1, keepdims=True) + UNIT_EPS
    )
    state_unit = jnp.einsum("shvk,shk->shv", head_state, unit_key)
    new_state = (
        head_state * decay_heads[:, :, None, :]
        - state_unit[..., None] * (unit_key * rate_heads)[:, :, None, :]
        + value_heads[..., None] * (key_heads * rate_heads)[:, :, None, :]
    )
    head_out = jnp.einsum("shvk,shk->shv", new_state, recept_heads)
    centre = jnp.mean(head_out, axis=-1, keepdims=True)
    spread = jnp.mean(jnp.square(head_out - centre), axis=-1, keepdims=True)
    normed_heads = (head_out - centre) * lax.rsqrt(spread + GROUP_EPS)
    mixed = (normed_heads.reshape(seq_count, -1) * head_gain).astype(jnp.bfloat16)
    return (new_state, mixed)


def expert_kernel(
    sizes,
    partial_ref,
    tokens_ref,
    routes_ref,
    weights_ref,
    gate_ref,
    up_ref,
    down_ref,
    out_ref,
    gu_vm,
    down_vm,
    info_out,
    info_in,
    part_in,
    resid,
    pick,
    mix_hi,
    mix_lo,
    z_out,
    z_in,
    y_in,
    share_out,
    share_in,
    back_out,
    back_in,
    mix_out,
    mix_in,
    load_sem,
    info_send,
    info_recv,
    part_send,
    part_recv,
    res_send,
    res_recv,
    z_send,
    z_recv,
    y_send,
    y_recv,
    share_send,
    share_recv,
    back_send,
    back_recv,
    mix_send,
    mix_recv,
):
    nz, nk, ny, seqs, width = sizes
    half = width // 2
    block = SLOTS * nk
    rows = nz * block
    groups = [range(g, min(g + GROUP, nz)) for g in range(0, nz, GROUP)]
    ep = lax.axis_index("ep")
    y = lax.axis_index("tp")
    z, k = ep // nk, ep % nk

    def in_z(j):
        return ((z + (plane_offset(j) + nz)) % nz) * nk + k, y

    def out_z(j):
        return ((z + (nz - plane_offset(j))) % nz) * nk + k, y

    def in_plane(q):
        return z * nk + (k + q) % nk, y

    def back_plane(q):
        return z * nk + (k + (nk - q)) % nk, y

    def in_y(q):
        return ep, (y + q) % ny

    def send(source, target, sends, receives, device):
        copy = pltpu.make_async_remote_copy(
            src_ref=source,
            dst_ref=target,
            send_sem=sends,
            recv_sem=receives,
            device_id=device,
            device_id_type=MESH,
        )
        copy.start()
        return copy

    barrier = pltpu.get_barrier_semaphore()
    peers = (
        [in_y(q) for q in range(1, ny)]
        + [in_plane(q) for q in range(1, nk)]
        + [in_z(j) for j in range(1, nz)]
    )
    for device in peers:
        pl.semaphore_signal(barrier, inc=1, device_id=device, device_id_type=MESH)

    loads = []
    for q in range(ny):
        own = pl.ds(pl.multiple_of(((y + (ny - q)) % ny) * width, LANES), width)
        put = pl.ds(q * width, width)
        hidden = gate_ref.shape[2]
        loads.append(
            pltpu.make_async_copy(
                gate_ref.at[0, own, :], gu_vm.at[put, pl.ds(0, hidden)], load_sem.at[0, q]
            )
        )
        loads.append(
            pltpu.make_async_copy(
                up_ref.at[0, own, :], gu_vm.at[put, pl.ds(hidden, hidden)], load_sem.at[1, q]
            )
        )
        ahead = pl.ds(pl.multiple_of(((y + q) % ny) * width, LANES), width)
        loads.append(
            pltpu.make_async_copy(
                down_ref.at[0, :, ahead], down_vm.at[:, pl.ds(q * width, width)], load_sem.at[2, q]
            )
        )
    for load in loads:
        load.start()

    count = nk * nz
    row = lax.broadcasted_iota(I32, (count, LANES), 0)
    j_of, q_of = row % nz, row // nz
    far = (j_of + 1) // 2
    away = jnp.where(j_of % 2 == 1, far, nz - far)
    expert = ((z + away) % nz) * nk + (k + q_of) % nk
    member = jnp.zeros((count, LANES), F32)
    weight = jnp.zeros((count, LANES), F32)
    for c in range(4):
        named = routes_ref[c : c + 1, :] == expert
        member = member + jnp.where(named, 1.0, 0.0)
        weight = weight + jnp.where(named, weights_ref[c : c + 1, :], 0.0)
    earlier_row = lax.broadcasted_iota(I32, (LANES, LANES), 0)
    later_row = lax.broadcasted_iota(I32, (LANES, LANES), 1)
    before = jnp.where(earlier_row < later_row, 1.0, 0.0).astype(BF16)
    earlier = jnp.dot(member.astype(BF16), before, preferred_element_type=F32)
    code = jnp.where(member > 0.5, earlier, 9.0)
    for q in range(nk):
        info_out[q, 0:nz, :] = code[q * nz : (q + 1) * nz]
        info_out[q, nz : 2 * nz, :] = weight[q * nz : (q + 1) * nz]

    resid[:, seqs:, :] = jnp.zeros((nk, LANES - seqs, width), BF16)

    pl.semaphore_wait(barrier, len(peers))

    flights = []
    arriving = {}
    for q in range(1, ny):
        copy = send(
            partial_ref.at[(y + q) % ny], part_in.at[q], part_send.at[q], part_recv.at[q], in_y(q)
        )
        arriving["part", q] = copy
        flights.append(copy)
    for q in range(1, nk):
        copy = send(info_out.at[q], info_in.at[q], info_send.at[q], info_recv.at[q], in_plane(q))
        arriving["info", q] = copy
        flights.append(copy)

    summed = partial_ref[y].astype(F32)
    for q in range(1, ny):
        arriving["part", q].wait_recv()
        summed = summed + part_in[q].astype(F32)
    residual = (tokens_ref[y].astype(F32) + summed).astype(BF16)
    resid[0, 0:seqs, :] = residual
    for q in range(1, nk):
        copy = send(
            resid.at[0, pl.ds(0, seqs)],
            resid.at[q, pl.ds(0, seqs)],
            res_send.at[q],
            res_recv.at[q],
            in_plane(q),
        )
        arriving["res", q] = copy
        flights.append(copy)

    rep_row = lax.broadcasted_iota(I32, (nz, SLOTS, nk, nz), 0).reshape(rows, nz)
    rep_col = lax.broadcasted_iota(I32, (nz, SLOTS, nk, nz), 3).reshape(rows, nz)
    repeat = jnp.where(rep_row == rep_col, 1.0, 0.0).astype(BF16)
    slot = lax.broadcasted_iota(I32, (nz, SLOTS, nk, LANES), 1).reshape(rows, LANES).astype(F32)
    source = lax.broadcasted_iota(I32, (nz, SLOTS, nk, LANES), 2).reshape(rows, LANES)
    for q in range(nk):
        if q:
            arriving["info", q].wait_recv()
        told = info_out if q == 0 else info_in
        spread = jnp.dot(repeat, told[q, 0:nz, :].astype(BF16), preferred_element_type=F32)
        chosen = jnp.where(spread == slot, jnp.where(source == q, 1.0, 0.0), 0.0)
        pick[:, q * LANES : (q + 1) * LANES] = chosen.astype(BF16)

    for q in range(1, nk):
        arriving["res", q].wait_recv()
    outgoing = jnp.dot(
        pick[...], resid[...].reshape(nk * LANES, width), preferred_element_type=F32
    ).reshape(nz, block, width)
    z_out[...] = jnp.concatenate([outgoing[:, :, :half], outgoing[:, :, half:]], axis=1).astype(BF16)

    for j in range(1, nz):
        copy = send(z_out.at[j], z_in.at[j], z_send.at[j], z_recv.at[j], in_z(j))
        arriving["z", j] = copy
        flights.append(copy)

    for q in range(nk):
        told = info_out if q == 0 else info_in
        weight = told[q, nz : 2 * nz, :]
        high = weight.astype(BF16)
        low = (weight - high.astype(F32)).astype(BF16)
        spread = jnp.dot(repeat, high, preferred_element_type=F32) + jnp.dot(
            repeat, low, preferred_element_type=F32
        )
        scaled = (spread * pick[:, q * LANES : (q + 1) * LANES].astype(F32)).T[0:seqs, :]
        high = scaled.astype(BF16)
        mix_hi[q] = high
        mix_lo[q] = (scaled - high.astype(F32)).astype(BF16)

    def forward(j):
        held = z_out.at[0] if j == 0 else z_in.at[j]
        if j:
            arriving["z", j].wait_recv()
        for q in range(1, ny):
            copy = send(held, y_in.at[q, j], y_send.at[q, j], y_recv.at[q, j], in_y(q))
            arriving["y", q, j] = copy
            flights.append(copy)

    def experts(group):
        columns = []
        for q in range(ny):
            pieces = []
            for j in group:
                if q:
                    arriving["y", q, j].wait_recv()
                    held = y_in[q, j]
                elif j:
                    held = z_in[j]
                else:
                    held = z_out[0]
                held = held.astype(F32)
                pieces.append(jnp.concatenate([held[:block], held[block:]], axis=1))
            columns.append(jnp.concatenate(pieces, axis=0))
        features = jnp.concatenate(columns, axis=1)
        normed = row_norm(features).astype(BF16)
        hidden = gu_vm.shape[1] // 2
        pre = jnp.dot(normed, gu_vm[...], preferred_element_type=F32)
        gated = jnp.minimum(pre[:, :hidden], CLAMP_LIMIT)
        linear = jnp.clip(pre[:, hidden:], -CLAMP_LIMIT, CLAMP_LIMIT)
        activated = (gated * jax.nn.sigmoid(GLU_ALPHA * gated) * (linear + 1.0)).astype(BF16)
        share = jnp.dot(activated, down_vm[...], preferred_element_type=F32)
        for q in range(ny):
            for at, j in enumerate(group):
                piece = share[at * block : (at + 1) * block, q * width : (q + 1) * width]
                share_out[q, j] = jnp.concatenate([piece[:, :half], piece[:, half:]], axis=0).astype(
                    BF16
                )
        for j in group:
            for q in range(1, ny):
                copy = send(
                    share_out.at[q, j],
                    share_in.at[q, j],
                    share_send.at[q, j],
                    share_recv.at[q, j],
                    in_y(q),
                )
                arriving["share", q, j] = copy
                flights.append(copy)

    def give_back(group):
        for j in group:
            total = share_out[0, j].astype(F32)
            for q in range(1, ny):
                arriving["share", q, j].wait_recv()
                total = total + share_in[q, j].astype(F32)
            total = total.astype(BF16)
            if j:
                back_out[j] = total
                copy = send(back_out.at[j], back_in.at[j], back_send.at[j], back_recv.at[j], out_z(j))
                arriving["back", j] = copy
                flights.append(copy)
            else:
                back_in[0] = total

    for g, group in enumerate(groups):
        for j in group:
            forward(j)
        if g == 0:
            for load in loads:
                load.wait()
        if g >= 1:
            experts(groups[g - 1])
        if g >= 2:
            give_back(groups[g - 2])
    experts(groups[-1])
    for group in groups[max(0, len(groups) - 2) :]:
        give_back(group)

    for j in range(1, nz):
        arriving["back", j].wait_recv()
    returned = back_in[...].astype(F32)
    returned = jnp.concatenate([returned[:, :block], returned[:, block:]], axis=2)
    returned = returned.reshape(rows, width).astype(BF16)
    mixture = jnp.dot(
        mix_hi[...].reshape(nk * seqs, rows), returned, preferred_element_type=F32
    ) + jnp.dot(mix_lo[...].reshape(nk * seqs, rows), returned, preferred_element_type=F32)
    mix_out[...] = mixture.reshape(nk, seqs, width).astype(BF16)
    for q in range(1, nk):
        copy = send(mix_out.at[q], mix_in.at[q], mix_send.at[q], mix_recv.at[q], back_plane(q))
        arriving["mix", q] = copy
        flights.append(copy)
    total = mixture[0:seqs]
    for q in range(1, nk):
        arriving["mix", q].wait_recv()
        total = total + mix_in[q].astype(F32)
    out_ref[...] = (resid[0, 0:seqs, :].astype(F32) + total).astype(BF16)
    for copy in flights:
        copy.wait_send()


def run_experts(sizes, partial, tokens, routes, weights, gate, up, down):
    nz, nk, ny, seqs, width = sizes
    rows = nz * SLOTS * nk
    message = (2 * SLOTS * nk, width // 2)
    hidden = gate.shape[2]
    dma = pltpu.SemaphoreType.DMA
    vmem = pl.BlockSpec(memory_space=pltpu.VMEM)
    hbm = pl.BlockSpec(memory_space=pl.ANY)
    scratch = [
        pltpu.VMEM((ny * width, 2 * hidden), BF16),
        pltpu.VMEM((hidden, ny * width), BF16),
        pltpu.VMEM((nk, 2 * nz, LANES), F32),
        pltpu.VMEM((nk, 2 * nz, LANES), F32),
        pltpu.VMEM((ny, seqs, width), BF16),
        pltpu.VMEM((nk, LANES, width), BF16),
        pltpu.VMEM((rows, nk * LANES), BF16),
        pltpu.VMEM((nk, seqs, rows), BF16),
        pltpu.VMEM((nk, seqs, rows), BF16),
        pltpu.VMEM((nz, *message), BF16),
        pltpu.VMEM((nz, *message), BF16),
        pltpu.VMEM((ny, nz, *message), BF16),
        pltpu.VMEM((ny, nz, *message), BF16),
        pltpu.VMEM((ny, nz, *message), BF16),
        pltpu.VMEM((nz, *message), BF16),
        pltpu.VMEM((nz, *message), BF16),
        pltpu.VMEM((nk, seqs, width), BF16),
        pltpu.VMEM((nk, seqs, width), BF16),
        dma((3, ny)),
    ]
    for shape in ((nk,), (ny,), (nk,), (nz,), (ny, nz), (ny, nz), (nz,), (nk,)):
        scratch += [dma(shape), dma(shape)]
    return pl.pallas_call(
        functools.partial(expert_kernel, sizes),
        out_shape=jax.ShapeDtypeStruct((seqs, width), BF16),
        in_specs=[vmem] * 4 + [hbm] * 3,
        out_specs=vmem,
        scratch_shapes=scratch,
        compiler_params=pltpu.CompilerParams(
            collective_id=0, has_side_effects=True, vmem_limit_bytes=40 * 1024 * 1024
        ),
        name="experts",
    )(partial, tokens, routes, weights, gate, up, down)


def local(
    tokens,
    head_state,
    recept_weight,
    key_weight,
    value_weight,
    decay_down_factor,
    decay_up_factor,
    decay_base,
    rate_down_factor,
    rate_up_factor,
    rate_base,
    head_gain,
    out_weight,
    route_experts,
    route_weights,
    expert_gate,
    expert_up,
    expert_down,
):
    tokens_float = tokens.astype(jnp.float32)
    normed = row_norm(tokens_float).astype(jnp.bfloat16)
    recept = jnp.dot(normed, recept_weight, preferred_element_type=jnp.float32).astype(jnp.bfloat16)
    keys = jnp.dot(normed, key_weight, preferred_element_type=jnp.float32).astype(jnp.bfloat16)
    values = jnp.dot(normed, value_weight, preferred_element_type=jnp.float32).astype(jnp.bfloat16)
    decay_low = jnp.tanh(
        jnp.dot(normed, decay_down_factor, preferred_element_type=jnp.float32)
    ).astype(jnp.bfloat16)
    rate_low = jnp.dot(normed, rate_down_factor, preferred_element_type=jnp.float32).astype(
        jnp.bfloat16
    )
    decay_pre = decay_base + jnp.dot(decay_low, decay_up_factor, preferred_element_type=jnp.float32)
    decay_rate = jnp.exp(-jnp.exp(-jax.nn.softplus(-decay_pre) - 0.5))
    rate_gate = jax.nn.sigmoid(
        rate_base + jnp.dot(rate_low, rate_up_factor, preferred_element_type=jnp.float32)
    )
    new_state, mixed = update_heads(
        head_state, recept, keys, values, decay_rate, rate_gate, head_gain
    )
    partial_value = jnp.dot(mixed, out_weight, preferred_element_type=jnp.float32).astype(
        jnp.bfloat16
    )
    ny = lax.axis_size("tp")
    nz = lax.axis_size("ep") // PLANE
    seqs, model = tokens.shape
    width = model // ny

    def by_columns(value):
        return value.reshape(seqs, ny, width).transpose(1, 0, 2)

    def by_lanes(value, fill):
        return jnp.pad(
            value.T, ((0, 8 - value.shape[1]), (0, LANES - seqs)), constant_values=fill
        )

    layer_out = run_experts(
        (nz, PLANE, ny, seqs, width),
        by_columns(partial_value),
        by_columns(tokens),
        by_lanes(route_experts, -1),
        by_lanes(route_weights, 0.0),
        expert_gate,
        expert_up,
        expert_down,
    )
    return (layer_out, new_state)


def solution(mesh):
    in_specs = (
        P("ep", None),
        P("ep", "tp", None, None),
        P(None, "tp"),
        P(None, "tp"),
        P(None, "tp"),
        P(),
        P(None, "tp"),
        P("tp"),
        P(),
        P(None, "tp"),
        P("tp"),
        P("tp"),
        P("tp", None),
        P("ep", None),
        P("ep", None),
        P("ep", None, "tp"),
        P("ep", None, "tp"),
        P("ep", "tp", None),
    )
    out_specs = (P("ep", "tp"), P("ep", "tp", None, None))
    return jax.shard_map(local, mesh=mesh, in_specs=in_specs, out_specs=out_specs, check_vma=False)
```

```python
import contextlib
import functools
import types

import jax
import jax.numpy as jnp
from jax import lax
from jax.experimental import pallas as pl
from jax.experimental.pallas import tpu as pltpu
from jax.sharding import PartitionSpec as P

NORM_EPS = 1e-05
GROUP_EPS = 0.00064
UNIT_EPS = 1e-06
CLAMP_LIMIT = 7.0
GLU_ALPHA = 1.702
PLANE = 8
SLOTS = 3
LANES = 128
GROUP = 4
PIECES = 6
SCOPES = False
MESH = pl.DeviceIdType.MESH
F32, BF16, I32 = jnp.float32, jnp.bfloat16, jnp.int32


def plane_offsets(nz):
    if nz == 16:
        return [0, 1, -1, 2, -2, 3, -3, 8, 7, -7, 6, -6, 5, -5, 4, -4]
    return [0] + [way * d for d in range(1, nz // 2) for way in (1, -1)] + [nz // 2]


def send_order(nz):
    offsets = plane_offsets(nz)
    ranked = sorted(range(1, nz), key=lambda j: -abs(offsets[j]))
    order = []
    while ranked:
        order.append(ranked.pop(0))
        if ranked:
            order.append(ranked.pop())
    return order


def scope(name):
    return jax.named_scope(name) if SCOPES else contextlib.nullcontext()


def row_norm(values):
    return values * lax.rsqrt(jnp.mean(values * values, axis=-1, keepdims=True) + NORM_EPS)


def dot(a, b):
    return jnp.dot(a, b, preferred_element_type=F32)


def dot_last(a, b):
    return lax.dot_general(a, b, (((1,), (1,)), ((), ())), preferred_element_type=F32)


INPUTS = [
    "tokens",
    "state",
    "recept",
    "key",
    "value",
    "decay_down",
    "decay_up",
    "decay_base",
    "rate_down",
    "rate_up",
    "rate_base",
    "gain",
    "out_weight",
    "routes",
    "weights",
    "gate",
    "up",
    "down",
]


def layer_kernel(sizes, names, *refs):
    nz, nk, ny, seqs, width = sizes
    r = types.SimpleNamespace(**dict(zip(names, refs, strict=True)))
    half = width // 2
    block = SLOTS * nk
    rows = nz * block
    groups = [range(g, min(g + GROUP, nz)) for g in range(0, nz, GROUP)]
    ep = lax.axis_index("ep")
    y = lax.axis_index("tp")
    z, k = ep // nk, ep % nk

    offsets = [offset % nz for offset in plane_offsets(nz)]

    def in_z(j):
        return ((z + offsets[j]) % nz) * nk + k, y

    def out_z(j):
        return ((z + (nz - offsets[j])) % nz) * nk + k, y

    def in_plane(q):
        return z * nk + (k + q) % nk, y

    def back_plane(q):
        return z * nk + (k + (nk - q)) % nk, y

    def in_y(q):
        return ep, (y + q) % ny

    def send(source, target, sends, receives, device):
        pltpu.make_async_remote_copy(
            src_ref=source,
            dst_ref=target,
            send_sem=sends,
            recv_sem=receives,
            device_id=device,
            device_id_type=MESH,
        ).start()

    def settle(ref, sem):
        pltpu.make_async_copy(ref, ref, sem).wait()

    barrier = pltpu.get_barrier_semaphore()
    peers = (
        [in_z(j) for j in range(nz - 1, 0, -1)]
        + [in_plane(q) for q in range(1, nk)]
        + [in_y(q) for q in range(1, ny)]
    )
    for device in peers:
        pl.semaphore_signal(barrier, inc=1, device_id=device, device_id_type=MESH)

    order = ["tokens", "low", "qkv", "up", "rows", "out", "gu", "down", "routes"]
    load_sem = {name: r.load_sem.at[i] for i, name in enumerate(order)}
    for s in range(0, seqs, 8):
        load_sem[s] = r.load_sem.at[len(order) + s // 8]

    def load(name, source, target):
        pltpu.make_async_copy(source, target, load_sem[name]).start()

    wide = r.recept.shape[1]
    low = r.decay_down.shape[0]
    heads = r.state.shape[1]
    head = wide // heads
    load("routes", r.routes, r.routes_vm)
    load("routes", r.weights, r.weights_vm)
    load("tokens", r.tokens, r.tokens_vm)
    load("low", r.decay_down, r.low_vm.at[pl.ds(0, low)])
    load("low", r.rate_down, r.low_vm.at[pl.ds(low, low)])
    load("qkv", r.recept, r.qkv_vm.at[:, pl.ds(0, wide)])
    load("qkv", r.key, r.qkv_vm.at[:, pl.ds(wide, wide)])
    load("qkv", r.value, r.qkv_vm.at[:, pl.ds(2 * wide, wide)])
    load("up", r.decay_up, r.up_vm.at[pl.ds(0, low), pl.ds(0, wide)])
    load("up", r.rate_up, r.up_vm.at[pl.ds(low, low), pl.ds(wide, wide)])
    load("rows", r.decay_base, r.base_vm)
    load("rows", r.rate_base, r.rate_vm)
    load("rows", r.gain, r.gain_vm)
    for s in range(0, seqs, 8):
        load(s, r.state.at[pl.ds(s, 8)], r.new_state.at[pl.ds(s, 8)])
    load("out", r.out_weight, r.out_vm)
    hidden = r.gate.shape[2]
    for q in range(ny):
        own = pl.ds(pl.multiple_of(((y + (ny - q)) % ny) * width, LANES), width)
        put = pl.ds(q * width, width)
        load("gu", r.gate.at[0, own, :], r.gu_vm.at[put, pl.ds(0, hidden)])
        load("gu", r.up.at[0, own, :], r.gu_vm.at[put, pl.ds(hidden, hidden)])
    for q in range(ny):
        ahead = pl.ds(pl.multiple_of(((y + q) % ny) * width, LANES), width)
        load("down", r.down.at[0, :, ahead], r.down_vm.at[:, pl.ds(q * width, width)])

    with scope("tables"):
        count = nk * nz
        row = lax.broadcasted_iota(I32, (count, seqs), 0)
        j_of, q_of = row % nz, row // nz
        away = jnp.zeros((count, seqs), I32)
        for j, offset in enumerate(offsets):
            away = jnp.where(j_of == j, offset, away)
        expert = ((z + away) % nz) * nk + (k + q_of) % nk
        member = jnp.zeros((count, seqs), F32)
        weight = jnp.zeros((count, seqs), F32)
        settle(r.routes_vm, load_sem["routes"])
        settle(r.weights_vm, load_sem["routes"])
        for c in range(r.routes.shape[0]):
            named = r.routes_vm[c : c + 1, :] == expert
            member = member + jnp.where(named, 1.0, 0.0)
            weight = weight + jnp.where(named, r.weights_vm[c : c + 1, :], 0.0)
        earlier_row = lax.broadcasted_iota(I32, (seqs, seqs), 0)
        later_row = lax.broadcasted_iota(I32, (seqs, seqs), 1)
        before = jnp.where(earlier_row < later_row, 1.0, 0.0).astype(BF16)
        earlier = dot(member.astype(BF16), before)
        code = jnp.where(member > 0.5, earlier, 9.0)
        r.info_out[...] = jnp.full(r.info_out.shape, 9.0, F32)
        for q in range(nk):
            r.info_out[q, 0:nz, 0:seqs] = code[q * nz : (q + 1) * nz]
            r.info_out[q, nz : 2 * nz, 0:seqs] = weight[q * nz : (q + 1) * nz]
        r.resid[:, seqs:, :] = jnp.zeros((nk, LANES - seqs, width), BF16)
        r.up_vm[0:low, wide:] = jnp.zeros((low, wide), BF16)
        r.up_vm[low:, 0:wide] = jnp.zeros((low, wide), BF16)

    with scope("project"):
        settle(r.tokens_vm, load_sem["tokens"])
        normed = row_norm(r.tokens_vm[...].astype(F32)).astype(BF16)
        settle(r.low_vm, load_sem["low"])
        lowered = dot_last(normed, r.low_vm[...])
        lane = lax.broadcasted_iota(I32, (seqs, 2 * low), 1)
        lowered = jnp.where(lane < low, jnp.tanh(lowered), lowered).astype(BF16)
        settle(r.qkv_vm, load_sem["qkv"])
        qkv = dot(normed, r.qkv_vm[...]).astype(BF16).astype(F32)
        recept, keys, values = qkv[:, :wide], qkv[:, wide : 2 * wide], qkv[:, 2 * wide :]
        settle(r.up_vm.at[pl.ds(0, low)], load_sem["up"])
        for ref in (r.base_vm, r.rate_vm, r.gain_vm):
            settle(ref, load_sem["rows"])
        raised = dot(lowered, r.up_vm[...])
        decay = jnp.exp(
            -jax.nn.sigmoid(raised[:, :wide] + r.base_vm[...]) * 0.6065306597126334
        )
        rate = jax.nn.sigmoid(raised[:, wide:] + r.rate_vm[...])

    lane = lax.broadcasted_iota(I32, (seqs, wide), 1)

    def head_sum(operand):
        total = jnp.zeros((seqs, wide), F32)
        for h in range(heads):
            mine = lane // head == h
            part = jnp.sum(jnp.where(mine, operand, 0.0), axis=1, keepdims=True)
            total = jnp.where(mine, part, total)
        return total

    with scope("heads"):
        unit = keys * lax.rsqrt(head_sum(keys * keys) + UNIT_EPS)
        unit_rate, key_rate = unit * rate, keys * rate

        def first_lanes(operand, h):
            return pltpu.roll(operand, wide - head * h, 1) if h else operand

        for h in range(heads):
            r.vec_vm[3 * h] = first_lanes(decay, h)
            r.vec_vm[3 * h + 1] = first_lanes(unit_rate, h)
            r.vec_vm[3 * h + 2] = first_lanes(key_rate, h)
        probes = [first_lanes(unit, h)[:, :head] for h in range(heads)]
        decayed = decay * recept
        probes += [first_lanes(decayed, h)[:, :head] for h in range(heads)]
        row8 = lax.broadcasted_iota(I32, (8, wide), 0)
        lane8 = lax.broadcasted_iota(I32, (8, wide), 1)
        found = [[], []]
        for s in range(0, seqs, 8):
            settle(r.new_state.at[pl.ds(s, 8)], load_sem[s])
            left = jnp.concatenate([probe[s : s + 8] for probe in probes], axis=0).astype(BF16)
            right = r.new_state[s : s + 8].reshape(8 * wide, head).astype(BF16)
            product = dot_last(left, right)
            for what in range(2):
                total = jnp.zeros((8, wide), F32)
                for h in range(heads):
                    at = (what * heads + h) * 8
                    for i in range(8):
                        here = jnp.logical_and(row8 == i, lane8 // head == h)
                        total = jnp.where(
                            here, product[at : at + 8, i * wide : (i + 1) * wide], total
                        )
                found[what].append(total)
        state_unit = jnp.concatenate(found[0], axis=0)
        head_out = (
            jnp.concatenate(found[1], axis=0)
            - state_unit * head_sum(unit_rate * recept)
            + values * head_sum(key_rate * recept)
        )
        r.col_vm[0] = state_unit
        r.col_vm[1] = values
        centred = head_out - head_sum(head_out) * (1.0 / head)
        spread = head_sum(centred * centred) * (1.0 / head)
        mixed = (centred * lax.rsqrt(spread + GROUP_EPS) * r.gain_vm[...]).astype(BF16)
        settle(r.out_vm, load_sem["out"])
        partial = dot(mixed, r.out_vm[...])
        for q in range(ny):
            r.part_out[q] = partial[:, q * width : (q + 1) * width].astype(BF16)

    with scope("barrier"):
        pl.semaphore_wait(barrier, len(peers))

    for q in range(1, ny):
        send(
            r.part_out.at[(y + q) % ny],
            r.part_in.at[q],
            r.part_send.at[0],
            r.part_recv.at[0],
            in_y(q),
        )
    for q in range(1, nk):
        send(r.info_out.at[q], r.info_in.at[q], r.info_send.at[0], r.info_recv.at[0], in_plane(q))

    with scope("reduce"):
        summed = r.part_out[y].astype(F32)
        settle(r.part_in.at[pl.ds(1, ny - 1)], r.part_recv.at[0])
        for q in range(1, ny):
            summed = summed + r.part_in[q].astype(F32)
        own = r.tokens_vm[:, pl.ds(pl.multiple_of(y * width, LANES), width)]
        r.resid[0, 0:seqs, :] = (own.astype(F32) + summed).astype(BF16)
    for q in range(1, nk):
        send(
            r.resid.at[0, pl.ds(0, seqs)],
            r.resid.at[q, pl.ds(0, seqs)],
            r.res_send.at[0],
            r.res_recv.at[0],
            in_plane(q),
        )

    with scope("pick"):
        rep_row = lax.broadcasted_iota(I32, (nz, SLOTS, nk, nz), 0).reshape(rows, nz)
        rep_col = lax.broadcasted_iota(I32, (nz, SLOTS, nk, nz), 3).reshape(rows, nz)
        repeat = jnp.where(rep_row == rep_col, 1.0, 0.0).astype(BF16)
        slot = lax.broadcasted_iota(I32, (nz, SLOTS, nk, LANES), 1).reshape(rows, LANES).astype(F32)
        source = lax.broadcasted_iota(I32, (nz, SLOTS, nk, LANES), 2).reshape(rows, LANES)
        settle(r.info_in.at[pl.ds(1, nk - 1)], r.info_recv.at[0])
        for q in range(nk):
            told = r.info_in if q else r.info_out
            spread = dot(repeat, told[q, 0:nz, :].astype(BF16))
            chosen = jnp.where(spread == slot, jnp.where(source == q, 1.0, 0.0), 0.0)
            r.pick[:, q * LANES : (q + 1) * LANES] = chosen.astype(BF16)

    with scope("gather"):
        settle(r.resid.at[pl.ds(1, nk - 1), pl.ds(0, seqs)], r.res_recv.at[0])
    with scope("dispatch"):
        outgoing = dot(r.pick[...], r.resid[...].reshape(nk * LANES, width))
        outgoing = outgoing.reshape(nz, block, width)
        r.z_out[...] = jnp.concatenate(
            [outgoing[:, :, :half], outgoing[:, :, half:]], axis=1
        ).astype(BF16)

    for j in send_order(nz):
        send(r.z_out.at[j], r.z_in.at[j], r.z_send.at[0], r.z_recv.at[j], in_z(j))

    def forward(j):
        held = r.z_in.at[j] if j else r.z_out.at[0]
        if j:
            settle(held, r.z_recv.at[j])
        for q in range(1, ny):
            send(held, r.y_in.at[q, j], r.y_send.at[0], r.y_recv.at[j // GROUP], in_y(q))

    def forward_group(group):
        for j in group:
            if j:
                forward(j)

    def load_experts(group):
        settle(r.gu_vm, load_sem["gu"])
        settle(r.down_vm, load_sem["down"])

    forward(0)

    def experts(group):
        at = (pl.ds(1, ny - 1), pl.ds(group[0], len(group)))
        settle(r.y_in.at[at], r.y_recv.at[group[0] // GROUP])
        columns = []
        for q in range(ny):
            pieces = []
            for j in group:
                if q:
                    held = r.y_in[q, j]
                elif j:
                    held = r.z_in[j]
                else:
                    held = r.z_out[0]
                held = held.astype(F32)
                pieces.append(jnp.concatenate([held[:block], held[block:]], axis=1))
            columns.append(jnp.concatenate(pieces, axis=0))
        features = jnp.concatenate(columns, axis=1)
        normed = row_norm(features).astype(BF16)
        pre = dot(normed, r.gu_vm[...])
        gated = jnp.minimum(pre[:, :hidden], CLAMP_LIMIT)
        linear = jnp.clip(pre[:, hidden:], -CLAMP_LIMIT, CLAMP_LIMIT)
        activated = (gated * jax.nn.sigmoid(GLU_ALPHA * gated) * (linear + 1.0)).astype(BF16)
        share = dot(activated, r.down_vm[...])
        for q in range(ny):
            for at, j in enumerate(group):
                piece = share[at * block : (at + 1) * block, q * width : (q + 1) * width]
                r.share_out[q, j] = jnp.concatenate(
                    [piece[:, :half], piece[:, half:]], axis=0
                ).astype(BF16)
        for j in group:
            for q in range(1, ny):
                send(
                    r.share_out.at[q, j],
                    r.share_in.at[q, j],
                    r.share_send.at[0],
                    r.share_recv.at[j // GROUP],
                    in_y(q),
                )

    def give_back(group):
        at = (pl.ds(1, ny - 1), pl.ds(group[0], len(group)))
        settle(r.share_in.at[at], r.share_recv.at[group[0] // GROUP])
        for j in group:
            total = r.share_out[0, j].astype(F32)
            for q in range(1, ny):
                total = total + r.share_in[q, j].astype(F32)
            total = total.astype(BF16)
            if j:
                r.back_out[j] = total
                send(
                    r.back_out.at[j], r.back_in.at[j], r.back_send.at[0], r.back_recv.at[0], out_z(j)
                )
            else:
                r.back_in[0] = total

    last = len(groups) - 1
    steps = []
    for g in range(last + 1):
        steps.append((forward_group, g))
        if g == last - 1:
            steps.append((load_experts, g))
            steps.append((experts, 0))
    for g in range(1 if last else 0, last + 1):
        steps.append((experts, g))
        if g >= 2:
            steps.append((give_back, g - 2))
    steps += [(give_back, g) for g in range(max(0, last - 1), last)]
    if not last:
        steps.insert(1, (load_experts, 0))
    for step, g in steps:
        with scope(f"{step.__name__}{g}"):
            step(groups[g])
    with scope("weights"):
        for q in range(nk):
            told = r.info_in if q else r.info_out
            weight = told[q, nz : 2 * nz, :]
            high = weight.astype(BF16)
            low_part = (weight - high.astype(F32)).astype(BF16)
            spread = dot(repeat, high) + dot(repeat, low_part)
            scaled = (spread * r.pick[:, q * LANES : (q + 1) * LANES].astype(F32)).T[0:seqs, :]
            high = scaled.astype(BF16)
            r.mix_hi[q] = high
            r.mix_lo[q] = (scaled - high.astype(F32)).astype(BF16)
    with scope("back_last"):
        give_back(groups[last])
    with scope("state"):
        for s in range(0, seqs, 8):
            lost = r.col_vm[0, s : s + 8, :].T
            gained = r.col_vm[1, s : s + 8, :].T
            for i in range(8):
                for h in range(heads):
                    at = pl.ds(s + i, 1)
                    span = slice(h * head, (h + 1) * head)
                    r.new_state[s + i, h] = (
                        r.new_state[s + i, h] * r.vec_vm[3 * h, at, :][:, :head]
                        - lost[span, i : i + 1] * r.vec_vm[3 * h + 1, at, :][:, :head]
                        + gained[span, i : i + 1] * r.vec_vm[3 * h + 2, at, :][:, :head]
                    )

    with scope("returned"):
        settle(r.back_in.at[pl.ds(1, nz - 1)], r.back_recv.at[0])
    with scope("mix"):
        returned = r.back_in[...].astype(F32)
        returned = jnp.concatenate([returned[:, :block], returned[:, block:]], axis=2)
        returned = returned.reshape(rows, width).astype(BF16)
        mixture = dot(r.mix_hi[...].reshape(nk * seqs, rows), returned) + dot(
            r.mix_lo[...].reshape(nk * seqs, rows), returned
        )
        r.mix_out[...] = mixture.reshape(nk, seqs, width).astype(BF16)
    for q in range(1, nk):
        send(r.mix_out.at[q], r.mix_in.at[q], r.mix_send.at[0], r.mix_recv.at[0], back_plane(q))
    with scope("final"):
        total = mixture[0:seqs]
        settle(r.mix_in.at[pl.ds(1, nk - 1)], r.mix_recv.at[0])
        for q in range(1, nk):
            total = total + r.mix_in[q].astype(F32)
        r.layer_out[...] = (r.resid[0, 0:seqs, :].astype(F32) + total).astype(BF16)
    with scope("drain"):
        settle(r.part_in.at[pl.ds(1, ny - 1)], r.part_send.at[0])
        settle(r.info_in.at[pl.ds(1, nk - 1)], r.info_send.at[0])
        settle(r.resid.at[pl.ds(1, nk - 1), pl.ds(0, seqs)], r.res_send.at[0])
        settle(r.z_in.at[pl.ds(1, nz - 1)], r.z_send.at[0])
        settle(r.y_in.at[pl.ds(1, ny - 1)], r.y_send.at[0])
        settle(r.share_in.at[pl.ds(1, ny - 1)], r.share_send.at[0])
        settle(r.back_in.at[pl.ds(1, nz - 1)], r.back_send.at[0])
        settle(r.mix_in.at[pl.ds(1, nk - 1)], r.mix_send.at[0])


def run_layer(sizes, *operands):
    nz, nk, ny, seqs, width = sizes
    args = dict(zip(INPUTS, operands, strict=True))
    rows = nz * SLOTS * nk
    message = (2 * SLOTS * nk, width // 2)
    hidden = args["gate"].shape[2]
    wide = args["recept"].shape[1]
    low = args["decay_down"].shape[0]
    state = args["state"].shape
    heads = state[1]
    dma = pltpu.SemaphoreType.DMA
    scratch = dict(
        tokens_vm=pltpu.VMEM((seqs, ny * width), BF16),
        qkv_vm=pltpu.VMEM((ny * width, 3 * wide), BF16),
        low_vm=pltpu.VMEM((2 * low, ny * width), BF16),
        up_vm=pltpu.VMEM((2 * low, 2 * wide), BF16),
        base_vm=pltpu.VMEM((1, wide), F32),
        rate_vm=pltpu.VMEM((1, wide), F32),
        gain_vm=pltpu.VMEM((1, wide), F32),
        routes_vm=pltpu.VMEM(args["routes"].shape, I32),
        weights_vm=pltpu.VMEM(args["weights"].shape, F32),
        vec_vm=pltpu.VMEM((3 * heads, seqs, wide), F32),
        col_vm=pltpu.VMEM((2, seqs, wide), F32),
        out_vm=pltpu.VMEM((wide, ny * width), BF16),
        gu_vm=pltpu.VMEM((ny * width, 2 * hidden), BF16),
        down_vm=pltpu.VMEM((hidden, ny * width), BF16),
        info_out=pltpu.VMEM((nk, 2 * nz, LANES), F32),
        info_in=pltpu.VMEM((nk, 2 * nz, LANES), F32),
        part_out=pltpu.VMEM((ny, seqs, width), BF16),
        part_in=pltpu.VMEM((ny, seqs, width), BF16),
        resid=pltpu.VMEM((nk, LANES, width), BF16),
        pick=pltpu.VMEM((rows, nk * LANES), BF16),
        mix_hi=pltpu.VMEM((nk, seqs, rows), BF16),
        mix_lo=pltpu.VMEM((nk, seqs, rows), BF16),
        z_out=pltpu.VMEM((nz, *message), BF16),
        z_in=pltpu.VMEM((nz, *message), BF16),
        y_in=pltpu.VMEM((ny, nz, *message), BF16),
        share_out=pltpu.VMEM((ny, nz, *message), BF16),
        share_in=pltpu.VMEM((ny, nz, *message), BF16),
        back_out=pltpu.VMEM((nz, *message), BF16),
        back_in=pltpu.VMEM((nz, *message), BF16),
        mix_out=pltpu.VMEM((nk, seqs, width), BF16),
        mix_in=pltpu.VMEM((nk, seqs, width), BF16),
        load_sem=dma((9 + seqs // 8,)),
    )
    waits = -(-nz // GROUP)
    for name, count in dict(
        info=1, part=1, res=1, z=nz, y=waits, share=waits, back=1, mix=1
    ).items():
        scratch[name + "_send"] = dma((1,))
        scratch[name + "_recv"] = dma((count,))
    hbm = pl.BlockSpec(memory_space=pltpu.HBM)
    vmem = pl.BlockSpec(memory_space=pltpu.VMEM)
    names = INPUTS + ["layer_out", "new_state"] + list(scratch)
    outs = ((seqs, width), BF16), (state, F32)
    results = pl.pallas_call(
        functools.partial(layer_kernel, sizes, names),
        out_shape=tuple(pltpu.VMEM(*out) for out in outs),
        in_specs=[hbm] * len(INPUTS),
        out_specs=(vmem, vmem),
        scratch_shapes=list(scratch.values()),
        compiler_params=pltpu.CompilerParams(
            collective_id=0, has_side_effects=True, vmem_limit_bytes=60 * 1024 * 1024
        ),
        name="layer",
    )(*operands)
    return pl.pallas_call(
        store_kernel,
        out_shape=tuple(jax.ShapeDtypeStruct(*out) for out in outs),
        in_specs=[vmem, vmem],
        out_specs=(hbm, hbm),
        scratch_shapes=[dma((PIECES + 1,))],
        compiler_params=pltpu.CompilerParams(vmem_limit_bytes=1024 * 1024),
        name="store",
    )(*results)


def store_kernel(layer_vm, state_vm, layer_ref, state_ref, sems):
    size = state_vm.shape[0] // PIECES
    copies = [pltpu.make_async_copy(layer_vm, layer_ref, sems.at[PIECES])]
    for i in range(PIECES):
        at = pl.ds(i * size, size)
        copies.append(pltpu.make_async_copy(state_vm.at[at], state_ref.at[at], sems.at[i]))
    for copy in copies:
        copy.start()
    for copy in copies:
        copy.wait()


def local(
    tokens,
    head_state,
    recept_weight,
    key_weight,
    value_weight,
    decay_down_factor,
    decay_up_factor,
    decay_base,
    rate_down_factor,
    rate_up_factor,
    rate_base,
    head_gain,
    out_weight,
    route_experts,
    route_weights,
    expert_gate,
    expert_up,
    expert_down,
):
    ny = lax.axis_size("tp")
    nz = lax.axis_size("ep") // PLANE
    seqs, model = tokens.shape

    return run_layer(
        (nz, PLANE, ny, seqs, model // ny),
        tokens,
        head_state,
        recept_weight,
        key_weight,
        value_weight,
        decay_down_factor.T,
        decay_up_factor,
        decay_base[None],
        rate_down_factor.T,
        rate_up_factor,
        rate_base[None],
        head_gain[None],
        out_weight,
        route_experts.T,
        route_weights.T,
        expert_gate,
        expert_up,
        expert_down,
    )


def solution(mesh):
    in_specs = (
        P("ep", None),
        P("ep", "tp", None, None),
        P(None, "tp"),
        P(None, "tp"),
        P(None, "tp"),
        P(),
        P(None, "tp"),
        P("tp"),
        P(),
        P(None, "tp"),
        P("tp"),
        P("tp"),
        P("tp", None),
        P("ep", None),
        P("ep", None),
        P("ep", None, "tp"),
        P("ep", None, "tp"),
        P("ep", "tp", None),
    )
    out_specs = (P("ep", "tp"), P("ep", "tp", None, None))
    return jax.shard_map(local, mesh=mesh, in_specs=in_specs, out_specs=out_specs, check_vma=False)
```

```python
import contextlib
import functools
import types

import jax
import jax.numpy as jnp
from jax import lax
from jax.experimental import pallas as pl
from jax.experimental.pallas import tpu as pltpu
from jax.sharding import PartitionSpec as P

NORM_EPS = 1e-05
GROUP_EPS = 0.00064
UNIT_EPS = 1e-06
CLAMP_LIMIT = 7.0
GLU_ALPHA = 1.702
PLANE = 8
SLOTS = 3
LANES = 128
WORK_ORDER = [0, 1, 2, 8, 7, 6, 5, 4, 3]
SEND_ORDER = [1, 2, 8, 7, 6, 5, 4, 3]
CUTS = [0, 3, 6, 10, 14, 16]
PLAN = ["F0", "L", "W", "F1", "E0", "F2", "F3", "F4", "E1", "E2", "B0", "E3", "B1", "E4", "B2", "B3", "B4"]
PIECES = 6
SCOPES = False
MESH = pl.DeviceIdType.MESH
F32, BF16, I32 = jnp.float32, jnp.bfloat16, jnp.int32


def plane_offsets(nz):
    if nz == 2 * len(WORK_ORDER) - 2:
        half = [way * d for d in WORK_ORDER for way in ((1, -1) if 0 < d < nz // 2 else (1,))]
        return half
    return [0] + [way * d for d in range(1, nz // 2) for way in (1, -1)] + [nz // 2]


def send_order(nz):
    offsets = plane_offsets(nz)
    if nz == 2 * len(SEND_ORDER):
        return [j for d in SEND_ORDER for j in range(nz) if abs(offsets[j]) == d]
    return list(range(1, nz))


def plane_groups(nz):
    cuts = CUTS if nz == 16 else [0, nz // 2, nz]
    return [range(low, high) for low, high in zip(cuts, cuts[1:])]


def plan(count):
    if count == len(CUTS) - 1:
        return PLAN
    steps = ["F0", "L"] + [f"F{g}" for g in range(1, count)] + [f"E{g}" for g in range(count)]
    return steps + [f"B{g}" for g in range(count)] + ["W"]


def scope(name):
    return jax.named_scope(name) if SCOPES else contextlib.nullcontext()


def row_norm(values):
    return values * lax.rsqrt(jnp.mean(values * values, axis=-1, keepdims=True) + NORM_EPS)


def dot(a, b):
    return jnp.dot(a, b, preferred_element_type=F32)


def dot_last(a, b):
    return lax.dot_general(a, b, (((1,), (1,)), ((), ())), preferred_element_type=F32)


INPUTS = [
    "tokens",
    "state",
    "recept",
    "key",
    "value",
    "decay_down",
    "decay_up",
    "decay_base",
    "rate_down",
    "rate_up",
    "rate_base",
    "gain",
    "out_weight",
    "routes",
    "weights",
    "gate",
    "up",
    "down",
]


def layer_kernel(sizes, names, *refs):
    nz, nk, ny, seqs, width = sizes
    r = types.SimpleNamespace(**dict(zip(names, refs, strict=True)))
    half = width // 2
    block = SLOTS * nk
    rows = nz * block
    groups = plane_groups(nz)
    group_of = {j: g for g, group in enumerate(groups) for j in group}
    ep = lax.axis_index("ep")
    y = lax.axis_index("tp")
    z, k = ep // nk, ep % nk

    offsets = [offset % nz for offset in plane_offsets(nz)]

    def in_z(j):
        return ((z + offsets[j]) % nz) * nk + k, y

    def out_z(j):
        return ((z + (nz - offsets[j])) % nz) * nk + k, y

    def in_plane(q):
        return z * nk + (k + q) % nk, y

    def back_plane(q):
        return z * nk + (k + (nk - q)) % nk, y

    def in_y(q):
        return ep, (y + q) % ny

    lanes = sorted(range(1, ny), key=lambda q: -min(q, ny - q))
    others = sorted(range(1, nk), key=lambda q: -min(q, nk - q))

    def send(source, target, sends, receives, device):
        pltpu.make_async_remote_copy(
            src_ref=source,
            dst_ref=target,
            send_sem=sends,
            recv_sem=receives,
            device_id=device,
            device_id_type=MESH,
        ).start()

    def settle(ref, sem):
        pltpu.make_async_copy(ref, ref, sem).wait()

    barrier = pltpu.get_barrier_semaphore()
    peers = (
        [in_z(j) for j in range(nz - 1, 0, -1)]
        + [in_plane(q) for q in range(1, nk)]
        + [in_y(q) for q in range(1, ny)]
    )
    for device in peers:
        pl.semaphore_signal(barrier, inc=1, device_id=device, device_id_type=MESH)

    order = ["tokens", "low", "qkv", "up", "rows", "out", "gu", "down", "routes"]
    load_sem = {name: r.load_sem.at[i] for i, name in enumerate(order)}
    for s in range(0, seqs, 8):
        load_sem[s] = r.load_sem.at[len(order) + s // 8]

    def load(name, source, target):
        pltpu.make_async_copy(source, target, load_sem[name]).start()

    wide = r.recept.shape[1]
    low = r.decay_down.shape[0]
    heads = r.state.shape[1]
    head = wide // heads
    load("routes", r.routes, r.routes_vm)
    load("routes", r.weights, r.weights_vm)
    load("tokens", r.tokens, r.tokens_vm)
    load("low", r.decay_down, r.low_vm.at[pl.ds(0, low)])
    load("low", r.rate_down, r.low_vm.at[pl.ds(low, low)])
    load("qkv", r.recept, r.qkv_vm.at[:, pl.ds(0, wide)])
    load("qkv", r.key, r.qkv_vm.at[:, pl.ds(wide, wide)])
    load("qkv", r.value, r.qkv_vm.at[:, pl.ds(2 * wide, wide)])
    load("up", r.decay_up, r.up_vm.at[pl.ds(0, low), pl.ds(0, wide)])
    load("up", r.rate_up, r.up_vm.at[pl.ds(low, low), pl.ds(wide, wide)])
    load("rows", r.decay_base, r.base_vm)
    load("rows", r.rate_base, r.rate_vm)
    load("rows", r.gain, r.gain_vm)
    for s in range(0, seqs, 8):
        load(s, r.state.at[pl.ds(s, 8)], r.new_state.at[pl.ds(s, 8)])
    load("out", r.out_weight, r.out_vm)
    hidden = r.gate.shape[2]
    for q in range(ny):
        own = pl.ds(pl.multiple_of(((y + (ny - q)) % ny) * width, LANES), width)
        put = pl.ds(q * width, width)
        load("gu", r.gate.at[0, own, :], r.gu_vm.at[put, pl.ds(0, hidden)])
        load("gu", r.up.at[0, own, :], r.gu_vm.at[put, pl.ds(hidden, hidden)])
    for q in range(ny):
        ahead = pl.ds(pl.multiple_of(((y + q) % ny) * width, LANES), width)
        load("down", r.down.at[0, :, ahead], r.down_vm.at[:, pl.ds(q * width, width)])

    with scope("tables"):
        count = nk * nz
        row = lax.broadcasted_iota(I32, (count, seqs), 0)
        j_of, q_of = row % nz, row // nz
        away = jnp.zeros((count, seqs), I32)
        for j, offset in enumerate(offsets):
            away = jnp.where(j_of == j, offset, away)
        expert = ((z + away) % nz) * nk + (k + q_of) % nk
        member = jnp.zeros((count, seqs), F32)
        weight = jnp.zeros((count, seqs), F32)
        settle(r.routes_vm, load_sem["routes"])
        settle(r.weights_vm, load_sem["routes"])
        for c in range(r.routes.shape[0]):
            named = r.routes_vm[c : c + 1, :] == expert
            member = member + jnp.where(named, 1.0, 0.0)
            weight = weight + jnp.where(named, r.weights_vm[c : c + 1, :], 0.0)
        earlier_row = lax.broadcasted_iota(I32, (seqs, seqs), 0)
        later_row = lax.broadcasted_iota(I32, (seqs, seqs), 1)
        before = jnp.where(earlier_row < later_row, 1.0, 0.0).astype(BF16)
        earlier = dot(member.astype(BF16), before)
        code = jnp.where(member > 0.5, earlier, 9.0)
        r.info_out[...] = jnp.full(r.info_out.shape, 9.0, F32)
        for q in range(nk):
            r.info_out[q, 0:nz, 0:seqs] = code[q * nz : (q + 1) * nz]
            r.info_out[q, nz : 2 * nz, 0:seqs] = weight[q * nz : (q + 1) * nz]
        r.resid[:, seqs:, :] = jnp.zeros((nk, LANES - seqs, width), BF16)
        r.up_vm[0:low, wide:] = jnp.zeros((low, wide), BF16)
        r.up_vm[low:, 0:wide] = jnp.zeros((low, wide), BF16)

    with scope("project"):
        settle(r.tokens_vm, load_sem["tokens"])
        normed = row_norm(r.tokens_vm[...].astype(F32)).astype(BF16)
        settle(r.low_vm, load_sem["low"])
        lowered = dot_last(normed, r.low_vm[...])
        lane = lax.broadcasted_iota(I32, (seqs, 2 * low), 1)
        lowered = jnp.where(lane < low, jnp.tanh(lowered), lowered).astype(BF16)
        settle(r.qkv_vm, load_sem["qkv"])
        qkv = dot(normed, r.qkv_vm[...]).astype(BF16).astype(F32)
        recept, keys, values = qkv[:, :wide], qkv[:, wide : 2 * wide], qkv[:, 2 * wide :]
        settle(r.up_vm.at[pl.ds(0, low)], load_sem["up"])
        for ref in (r.base_vm, r.rate_vm, r.gain_vm):
            settle(ref, load_sem["rows"])
        raised = dot(lowered, r.up_vm[...])
        decay = jnp.exp(
            -jax.nn.sigmoid(raised[:, :wide] + r.base_vm[...]) * 0.6065306597126334
        )
        rate = jax.nn.sigmoid(raised[:, wide:] + r.rate_vm[...])

    lane = lax.broadcasted_iota(I32, (seqs, wide), 1)

    def head_sum(operand):
        total = jnp.zeros((seqs, wide), F32)
        for h in range(heads):
            mine = lane // head == h
            part = jnp.sum(jnp.where(mine, operand, 0.0), axis=1, keepdims=True)
            total = jnp.where(mine, part, total)
        return total

    with scope("heads"):
        unit = keys * lax.rsqrt(head_sum(keys * keys) + UNIT_EPS)
        unit_rate, key_rate = unit * rate, keys * rate

        def first_lanes(operand, h):
            return pltpu.roll(operand, wide - head * h, 1) if h else operand

        for h in range(heads):
            r.vec_vm[3 * h] = first_lanes(decay, h)
            r.vec_vm[3 * h + 1] = first_lanes(unit_rate, h)
            r.vec_vm[3 * h + 2] = first_lanes(key_rate, h)
        probes = [first_lanes(unit, h)[:, :head] for h in range(heads)]
        decayed = decay * recept
        probes += [first_lanes(decayed, h)[:, :head] for h in range(heads)]
        row8 = lax.broadcasted_iota(I32, (8, wide), 0)
        lane8 = lax.broadcasted_iota(I32, (8, wide), 1)
        found = [[], []]
        for s in range(0, seqs, 8):
            settle(r.new_state.at[pl.ds(s, 8)], load_sem[s])
            left = jnp.concatenate([probe[s : s + 8] for probe in probes], axis=0).astype(BF16)
            right = r.new_state[s : s + 8].reshape(8 * wide, head).astype(BF16)
            product = dot_last(left, right)
            for what in range(2):
                total = jnp.zeros((8, wide), F32)
                for h in range(heads):
                    at = (what * heads + h) * 8
                    for i in range(8):
                        here = jnp.logical_and(row8 == i, lane8 // head == h)
                        total = jnp.where(
                            here, product[at : at + 8, i * wide : (i + 1) * wide], total
                        )
                found[what].append(total)
        state_unit = jnp.concatenate(found[0], axis=0)
        head_out = (
            jnp.concatenate(found[1], axis=0)
            - state_unit * head_sum(unit_rate * recept)
            + values * head_sum(key_rate * recept)
        )
        r.col_vm[0] = state_unit
        r.col_vm[1] = values
        centred = head_out - head_sum(head_out) * (1.0 / head)
        spread = head_sum(centred * centred) * (1.0 / head)
        mixed = (centred * lax.rsqrt(spread + GROUP_EPS) * r.gain_vm[...]).astype(BF16)
        settle(r.out_vm, load_sem["out"])
        partial = dot(mixed, r.out_vm[...])
        for q in range(ny):
            r.part_out[q] = partial[:, q * width : (q + 1) * width].astype(BF16)

    with scope("barrier"):
        pl.semaphore_wait(barrier, len(peers))

    for q in lanes:
        send(
            r.part_out.at[(y + q) % ny],
            r.part_in.at[q],
            r.part_send.at[0],
            r.part_recv.at[0],
            in_y(q),
        )
    for q in others:
        send(r.info_out.at[q], r.info_in.at[q], r.info_send.at[0], r.info_recv.at[0], in_plane(q))

    with scope("reduce"):
        summed = r.part_out[y].astype(F32)
        settle(r.part_in.at[pl.ds(1, ny - 1)], r.part_recv.at[0])
        for q in range(1, ny):
            summed = summed + r.part_in[q].astype(F32)
        own = r.tokens_vm[:, pl.ds(pl.multiple_of(y * width, LANES), width)]
        r.resid[0, 0:seqs, :] = (own.astype(F32) + summed).astype(BF16)
    for q in others:
        send(
            r.resid.at[0, pl.ds(0, seqs)],
            r.resid.at[q, pl.ds(0, seqs)],
            r.res_send.at[0],
            r.res_recv.at[0],
            in_plane(q),
        )

    with scope("pick"):
        rep_row = lax.broadcasted_iota(I32, (nz, SLOTS, nk, nz), 0).reshape(rows, nz)
        rep_col = lax.broadcasted_iota(I32, (nz, SLOTS, nk, nz), 3).reshape(rows, nz)
        repeat = jnp.where(rep_row == rep_col, 1.0, 0.0).astype(BF16)
        slot = lax.broadcasted_iota(I32, (nz, SLOTS, nk, LANES), 1).reshape(rows, LANES).astype(F32)
        source = lax.broadcasted_iota(I32, (nz, SLOTS, nk, LANES), 2).reshape(rows, LANES)
        settle(r.info_in.at[pl.ds(1, nk - 1)], r.info_recv.at[0])
        for q in range(nk):
            told = r.info_in if q else r.info_out
            spread = dot(repeat, told[q, 0:nz, :].astype(BF16))
            chosen = jnp.where(spread == slot, jnp.where(source == q, 1.0, 0.0), 0.0)
            r.pick[:, q * LANES : (q + 1) * LANES] = chosen.astype(BF16)

    with scope("gather"):
        settle(r.resid.at[pl.ds(1, nk - 1), pl.ds(0, seqs)], r.res_recv.at[0])
    with scope("dispatch"):
        outgoing = dot(r.pick[...], r.resid[...].reshape(nk * LANES, width))
        outgoing = outgoing.reshape(nz, block, width)
        r.z_out[...] = jnp.concatenate(
            [outgoing[:, :, :half], outgoing[:, :, half:]], axis=1
        ).astype(BF16)

    for j in send_order(nz):
        send(r.z_out.at[j], r.z_in.at[j], r.z_send.at[0], r.z_recv.at[j], in_z(j))

    def forward(source, group):
        span = pl.ds(group[0], len(group))
        for q in lanes:
            target = r.y_in.at[q, span]
            send(source.at[span], target, r.y_send.at[0], r.y_recv.at[group_of[group[0]]], in_y(q))

    def forward_group(group):
        group = [j for j in group if j]
        for j in group:
            settle(r.z_in.at[j], r.z_recv.at[j])
        if group:
            forward(r.z_in, group)

    forward(r.z_out, [0])

    def experts(group):
        at = (pl.ds(1, ny - 1), pl.ds(group[0], len(group)))
        settle(r.y_in.at[at], r.y_recv.at[group_of[group[0]]])
        columns = []
        for q in range(ny):
            pieces = []
            for j in group:
                if q:
                    held = r.y_in[q, j]
                elif j:
                    held = r.z_in[j]
                else:
                    held = r.z_out[0]
                held = held.astype(F32)
                pieces.append(jnp.concatenate([held[:block], held[block:]], axis=1))
            columns.append(jnp.concatenate(pieces, axis=0))
        features = jnp.concatenate(columns, axis=1)
        normed = row_norm(features).astype(BF16)
        pre = dot(normed, r.gu_vm[...])
        gated = jnp.minimum(pre[:, :hidden], CLAMP_LIMIT)
        linear = jnp.clip(pre[:, hidden:], -CLAMP_LIMIT, CLAMP_LIMIT)
        activated = (gated * jax.nn.sigmoid(GLU_ALPHA * gated) * (linear + 1.0)).astype(BF16)
        share = dot(activated, r.down_vm[...])
        for q in range(ny):
            for at, j in enumerate(group):
                piece = share[at * block : (at + 1) * block, q * width : (q + 1) * width]
                r.share_out[q, j] = jnp.concatenate(
                    [piece[:, :half], piece[:, half:]], axis=0
                ).astype(BF16)
        for q in lanes:
            at = (q, pl.ds(group[0], len(group)))
            g = group_of[group[0]]
            send(
                r.share_out.at[at], r.share_in.at[at], r.share_send.at[0], r.share_recv.at[g], in_y(q)
            )

    def give_back(group):
        at = (pl.ds(1, ny - 1), pl.ds(group[0], len(group)))
        settle(r.share_in.at[at], r.share_recv.at[group_of[group[0]]])
        for j in group:
            total = r.share_out[0, j].astype(F32)
            for q in range(1, ny):
                total = total + r.share_in[q, j].astype(F32)
            total = total.astype(BF16)
            if j:
                r.back_out[j] = total
                send(
                    r.back_out.at[j], r.back_in.at[j], r.back_send.at[0], r.back_recv.at[0], out_z(j)
                )
            else:
                r.back_in[0] = total

    def return_weights():
        for q in range(nk):
            told = r.info_in if q else r.info_out
            weight = told[q, nz : 2 * nz, :]
            high = weight.astype(BF16)
            low_part = (weight - high.astype(F32)).astype(BF16)
            spread = dot(repeat, high) + dot(repeat, low_part)
            scaled = (spread * r.pick[:, q * LANES : (q + 1) * LANES].astype(F32)).T[0:seqs, :]
            high = scaled.astype(BF16)
            r.mix_hi[q] = high
            r.mix_lo[q] = (scaled - high.astype(F32)).astype(BF16)

    for step in plan(len(groups)):
        with scope(step):
            if step == "L":
                settle(r.gu_vm, load_sem["gu"])
                settle(r.down_vm, load_sem["down"])
            elif step == "W":
                return_weights()
            else:
                work = dict(F=forward_group, E=experts, B=give_back)[step[0]]
                work(groups[int(step[1:])])
    with scope("state"):
        for s in range(0, seqs, 8):
            lost = r.col_vm[0, s : s + 8, :].T
            gained = r.col_vm[1, s : s + 8, :].T
            for i in range(8):
                for h in range(heads):
                    at = pl.ds(s + i, 1)
                    span = slice(h * head, (h + 1) * head)
                    r.new_state[s + i, h] = (
                        r.new_state[s + i, h] * r.vec_vm[3 * h, at, :][:, :head]
                        - lost[span, i : i + 1] * r.vec_vm[3 * h + 1, at, :][:, :head]
                        + gained[span, i : i + 1] * r.vec_vm[3 * h + 2, at, :][:, :head]
                    )

    with scope("returned"):
        settle(r.back_in.at[pl.ds(1, nz - 1)], r.back_recv.at[0])
    with scope("mix"):
        returned = r.back_in[...].astype(F32)
        returned = jnp.concatenate([returned[:, :block], returned[:, block:]], axis=2)
        returned = returned.reshape(rows, width).astype(BF16)
        mixture = dot(r.mix_hi[...].reshape(nk * seqs, rows), returned) + dot(
            r.mix_lo[...].reshape(nk * seqs, rows), returned
        )
        r.mix_out[...] = mixture.reshape(nk, seqs, width).astype(BF16)
    for q in others:
        send(r.mix_out.at[q], r.mix_in.at[q], r.mix_send.at[0], r.mix_recv.at[0], back_plane(q))
    with scope("final"):
        total = mixture[0:seqs]
        settle(r.mix_in.at[pl.ds(1, nk - 1)], r.mix_recv.at[0])
        for q in range(1, nk):
            total = total + r.mix_in[q].astype(F32)
        r.layer_out[...] = (r.resid[0, 0:seqs, :].astype(F32) + total).astype(BF16)
    with scope("drain"):
        settle(r.part_in.at[pl.ds(1, ny - 1)], r.part_send.at[0])
        settle(r.info_in.at[pl.ds(1, nk - 1)], r.info_send.at[0])
        settle(r.resid.at[pl.ds(1, nk - 1), pl.ds(0, seqs)], r.res_send.at[0])
        settle(r.z_in.at[pl.ds(1, nz - 1)], r.z_send.at[0])
        settle(r.y_in.at[pl.ds(1, ny - 1)], r.y_send.at[0])
        settle(r.share_in.at[pl.ds(1, ny - 1)], r.share_send.at[0])
        settle(r.back_in.at[pl.ds(1, nz - 1)], r.back_send.at[0])
        settle(r.mix_in.at[pl.ds(1, nk - 1)], r.mix_send.at[0])


def run_layer(sizes, *operands):
    nz, nk, ny, seqs, width = sizes
    args = dict(zip(INPUTS, operands, strict=True))
    rows = nz * SLOTS * nk
    message = (2 * SLOTS * nk, width // 2)
    hidden = args["gate"].shape[2]
    wide = args["recept"].shape[1]
    low = args["decay_down"].shape[0]
    state = args["state"].shape
    heads = state[1]
    dma = pltpu.SemaphoreType.DMA
    scratch = dict(
        tokens_vm=pltpu.VMEM((seqs, ny * width), BF16),
        qkv_vm=pltpu.VMEM((ny * width, 3 * wide), BF16),
        low_vm=pltpu.VMEM((2 * low, ny * width), BF16),
        up_vm=pltpu.VMEM((2 * low, 2 * wide), BF16),
        base_vm=pltpu.VMEM((1, wide), F32),
        rate_vm=pltpu.VMEM((1, wide), F32),
        gain_vm=pltpu.VMEM((1, wide), F32),
        routes_vm=pltpu.VMEM(args["routes"].shape, I32),
        weights_vm=pltpu.VMEM(args["weights"].shape, F32),
        vec_vm=pltpu.VMEM((3 * heads, seqs, wide), F32),
        col_vm=pltpu.VMEM((2, seqs, wide), F32),
        out_vm=pltpu.VMEM((wide, ny * width), BF16),
        gu_vm=pltpu.VMEM((ny * width, 2 * hidden), BF16),
        down_vm=pltpu.VMEM((hidden, ny * width), BF16),
        info_out=pltpu.VMEM((nk, 2 * nz, LANES), F32),
        info_in=pltpu.VMEM((nk, 2 * nz, LANES), F32),
        part_out=pltpu.VMEM((ny, seqs, width), BF16),
        part_in=pltpu.VMEM((ny, seqs, width), BF16),
        resid=pltpu.VMEM((nk, LANES, width), BF16),
        pick=pltpu.VMEM((rows, nk * LANES), BF16),
        mix_hi=pltpu.VMEM((nk, seqs, rows), BF16),
        mix_lo=pltpu.VMEM((nk, seqs, rows), BF16),
        z_out=pltpu.VMEM((nz, *message), BF16),
        z_in=pltpu.VMEM((nz, *message), BF16),
        y_in=pltpu.VMEM((ny, nz, *message), BF16),
        share_out=pltpu.VMEM((ny, nz, *message), BF16),
        share_in=pltpu.VMEM((ny, nz, *message), BF16),
        back_out=pltpu.VMEM((nz, *message), BF16),
        back_in=pltpu.VMEM((nz, *message), BF16),
        mix_out=pltpu.VMEM((nk, seqs, width), BF16),
        mix_in=pltpu.VMEM((nk, seqs, width), BF16),
        load_sem=dma((9 + seqs // 8,)),
    )
    waits = len(plane_groups(nz))
    for name, count in dict(
        info=1, part=1, res=1, z=nz, y=waits, share=waits, back=1, mix=1
    ).items():
        scratch[name + "_send"] = dma((1,))
        scratch[name + "_recv"] = dma((count,))
    hbm = pl.BlockSpec(memory_space=pltpu.HBM)
    vmem = pl.BlockSpec(memory_space=pltpu.VMEM)
    names = INPUTS + ["layer_out", "new_state"] + list(scratch)
    outs = ((seqs, width), BF16), (state, F32)
    results = pl.pallas_call(
        functools.partial(layer_kernel, sizes, names),
        out_shape=tuple(pltpu.VMEM(*out) for out in outs),
        in_specs=[hbm] * len(INPUTS),
        out_specs=(vmem, vmem),
        scratch_shapes=list(scratch.values()),
        compiler_params=pltpu.CompilerParams(
            collective_id=0, has_side_effects=True, vmem_limit_bytes=60 * 1024 * 1024
        ),
        name="layer",
    )(*operands)
    return pl.pallas_call(
        store_kernel,
        out_shape=tuple(jax.ShapeDtypeStruct(*out) for out in outs),
        in_specs=[vmem, vmem],
        out_specs=(hbm, hbm),
        scratch_shapes=[dma((PIECES + 1,))],
        compiler_params=pltpu.CompilerParams(vmem_limit_bytes=1024 * 1024),
        name="store",
    )(*results)


def store_kernel(layer_vm, state_vm, layer_ref, state_ref, sems):
    size = state_vm.shape[0] // PIECES
    copies = [pltpu.make_async_copy(layer_vm, layer_ref, sems.at[PIECES])]
    for i in range(PIECES):
        at = pl.ds(i * size, size)
        copies.append(pltpu.make_async_copy(state_vm.at[at], state_ref.at[at], sems.at[i]))
    for copy in copies:
        copy.start()
    for copy in copies:
        copy.wait()


def local(
    tokens,
    head_state,
    recept_weight,
    key_weight,
    value_weight,
    decay_down_factor,
    decay_up_factor,
    decay_base,
    rate_down_factor,
    rate_up_factor,
    rate_base,
    head_gain,
    out_weight,
    route_experts,
    route_weights,
    expert_gate,
    expert_up,
    expert_down,
):
    ny = lax.axis_size("tp")
    nz = lax.axis_size("ep") // PLANE
    seqs, model = tokens.shape

    return run_layer(
        (nz, PLANE, ny, seqs, model // ny),
        tokens,
        head_state,
        recept_weight,
        key_weight,
        value_weight,
        decay_down_factor.T,
        decay_up_factor,
        decay_base[None],
        rate_down_factor.T,
        rate_up_factor,
        rate_base[None],
        head_gain[None],
        out_weight,
        route_experts.T,
        route_weights.T,
        expert_gate,
        expert_up,
        expert_down,
    )


def solution(mesh):
    in_specs = (
        P("ep", None),
        P("ep", "tp", None, None),
        P(None, "tp"),
        P(None, "tp"),
        P(None, "tp"),
        P(),
        P(None, "tp"),
        P("tp"),
        P(),
        P(None, "tp"),
        P("tp"),
        P("tp"),
        P("tp", None),
        P("ep", None),
        P("ep", None),
        P("ep", None, "tp"),
        P("ep", None, "tp"),
        P("ep", "tp", None),
    )
    out_specs = (P("ep", "tp"), P("ep", "tp", None, None))
    return jax.shard_map(local, mesh=mesh, in_specs=in_specs, out_specs=out_specs, check_vma=False)
```

```python
import contextlib
import functools
import types

import jax
import jax.numpy as jnp
from jax import lax
from jax.experimental import pallas as pl
from jax.experimental.pallas import tpu as pltpu
from jax.sharding import PartitionSpec as P

NORM_EPS = 1e-05
GROUP_EPS = 0.00064
UNIT_EPS = 1e-06
CLAMP_LIMIT = 7.0
GLU_ALPHA = 1.702
PLANE = 8
SLOTS = 3
LANES = 128
WORK_ORDER = [0, 1, 2, 8, 7, 6, 5, 4, 3]
SEND_ORDER = [1, 2, 8, 7, 6, 5, 4, 3]
CUTS = [0, 3, 5, 9, 13, 16]
PLAN = ["F0", "L", "F1", "W", "E0", "E1", "F2", "F3", "F4", "B0", "B1", "E2", "E3", "E4", "B2", "B3", "B4"]
PIECES = 6
SCOPES = False
MESH = pl.DeviceIdType.MESH
F32, BF16, I32 = jnp.float32, jnp.bfloat16, jnp.int32


def plane_offsets(nz):
    if nz == 2 * len(WORK_ORDER) - 2:
        half = [way * d for d in WORK_ORDER for way in ((1, -1) if 0 < d < nz // 2 else (1,))]
        return half
    return [0] + [way * d for d in range(1, nz // 2) for way in (1, -1)] + [nz // 2]


def send_order(nz):
    offsets = plane_offsets(nz)
    if nz == 2 * len(SEND_ORDER):
        return [j for d in SEND_ORDER for j in range(nz) if abs(offsets[j]) == d]
    return list(range(1, nz))


def plane_groups(nz):
    cuts = CUTS if nz == 16 else [0, nz // 2, nz]
    return [range(low, high) for low, high in zip(cuts, cuts[1:])]


def plan(count):
    if count == len(CUTS) - 1:
        return PLAN
    steps = ["F0", "L"] + [f"F{g}" for g in range(1, count)] + [f"E{g}" for g in range(count)]
    return steps + [f"B{g}" for g in range(count)] + ["W"]


def scope(name):
    return jax.named_scope(name) if SCOPES else contextlib.nullcontext()


def row_norm(values):
    return values * lax.rsqrt(jnp.mean(values * values, axis=-1, keepdims=True) + NORM_EPS)


def dot(a, b):
    return jnp.dot(a, b, preferred_element_type=F32)


def dot_last(a, b):
    return lax.dot_general(a, b, (((1,), (1,)), ((), ())), preferred_element_type=F32)


INPUTS = [
    "tokens",
    "state",
    "recept",
    "key",
    "value",
    "decay_down",
    "decay_up",
    "decay_base",
    "rate_down",
    "rate_up",
    "rate_base",
    "gain",
    "out_weight",
    "routes",
    "weights",
    "gate",
    "up",
    "down",
]


def layer_kernel(sizes, names, *refs):
    nz, nk, ny, seqs, width = sizes
    r = types.SimpleNamespace(**dict(zip(names, refs, strict=True)))
    half = width // 2
    block = SLOTS * nk
    rows = nz * block
    groups = plane_groups(nz)
    group_of = {j: g for g, group in enumerate(groups) for j in group}
    ep = lax.axis_index("ep")
    y = lax.axis_index("tp")
    z, k = ep // nk, ep % nk

    offsets = [offset % nz for offset in plane_offsets(nz)]

    def in_z(j):
        return ((z + offsets[j]) % nz) * nk + k, y

    def out_z(j):
        return ((z + (nz - offsets[j])) % nz) * nk + k, y

    def in_plane(q):
        return z * nk + (k + q) % nk, y

    def back_plane(q):
        return z * nk + (k + (nk - q)) % nk, y

    def in_y(q):
        return ep, (y + q) % ny

    lanes = sorted(range(1, ny), key=lambda q: -min(q, ny - q))
    others = sorted(range(1, nk), key=lambda q: -min(q, nk - q))

    def send(source, target, sends, receives, device):
        pltpu.make_async_remote_copy(
            src_ref=source,
            dst_ref=target,
            send_sem=sends,
            recv_sem=receives,
            device_id=device,
            device_id_type=MESH,
        ).start()

    def settle(ref, sem):
        pltpu.make_async_copy(ref, ref, sem).wait()

    barrier = pltpu.get_barrier_semaphore()
    peers = (
        [in_z(j) for j in range(nz - 1, 0, -1)]
        + [in_plane(q) for q in range(1, nk)]
        + [in_y(q) for q in range(1, ny)]
    )
    for device in peers:
        pl.semaphore_signal(barrier, inc=1, device_id=device, device_id_type=MESH)

    order = ["tokens", "low", "qkv", "up", "rows", "out", "gu", "down", "routes"]
    load_sem = {name: r.load_sem.at[i] for i, name in enumerate(order)}
    for s in range(0, seqs, 8):
        load_sem[s] = r.load_sem.at[len(order) + s // 8]

    def load(name, source, target):
        pltpu.make_async_copy(source, target, load_sem[name]).start()

    wide = r.recept.shape[1]
    low = r.decay_down.shape[0]
    heads = r.state.shape[1]
    head = wide // heads
    load("routes", r.routes, r.routes_vm)
    load("routes", r.weights, r.weights_vm)
    load("tokens", r.tokens, r.tokens_vm)
    load("low", r.decay_down, r.low_vm.at[pl.ds(0, low)])
    load("low", r.rate_down, r.low_vm.at[pl.ds(low, low)])
    load("qkv", r.recept, r.qkv_vm.at[:, pl.ds(0, wide)])
    load("qkv", r.key, r.qkv_vm.at[:, pl.ds(wide, wide)])
    load("qkv", r.value, r.qkv_vm.at[:, pl.ds(2 * wide, wide)])
    load("up", r.decay_up, r.up_vm.at[pl.ds(0, low), pl.ds(0, wide)])
    load("up", r.rate_up, r.up_vm.at[pl.ds(low, low), pl.ds(wide, wide)])
    load("rows", r.decay_base, r.base_vm)
    load("rows", r.rate_base, r.rate_vm)
    load("rows", r.gain, r.gain_vm)
    for s in range(0, seqs, 8):
        load(s, r.state.at[pl.ds(s, 8)], r.new_state.at[pl.ds(s, 8)])
    load("out", r.out_weight, r.out_vm)
    hidden = r.gate.shape[2]
    for q in range(ny):
        own = pl.ds(pl.multiple_of(((y + (ny - q)) % ny) * width, LANES), width)
        put = pl.ds(q * width, width)
        load("gu", r.gate.at[0, own, :], r.gu_vm.at[put, pl.ds(0, hidden)])
        load("gu", r.up.at[0, own, :], r.gu_vm.at[put, pl.ds(hidden, hidden)])
    for q in range(ny):
        ahead = pl.ds(pl.multiple_of(((y + q) % ny) * width, LANES), width)
        load("down", r.down.at[0, :, ahead], r.down_vm.at[:, pl.ds(q * width, width)])

    with scope("tables"):
        count = nk * nz
        row = lax.broadcasted_iota(I32, (count, seqs), 0)
        j_of, q_of = row % nz, row // nz
        away = jnp.zeros((count, seqs), I32)
        for j, offset in enumerate(offsets):
            away = jnp.where(j_of == j, offset, away)
        expert = ((z + away) % nz) * nk + (k + q_of) % nk
        member = jnp.zeros((count, seqs), F32)
        weight = jnp.zeros((count, seqs), F32)
        settle(r.routes_vm, load_sem["routes"])
        settle(r.weights_vm, load_sem["routes"])
        for c in range(r.routes.shape[0]):
            named = r.routes_vm[c : c + 1, :] == expert
            member = member + jnp.where(named, 1.0, 0.0)
            weight = weight + jnp.where(named, r.weights_vm[c : c + 1, :], 0.0)
        earlier_row = lax.broadcasted_iota(I32, (seqs, seqs), 0)
        later_row = lax.broadcasted_iota(I32, (seqs, seqs), 1)
        before = jnp.where(earlier_row < later_row, 1.0, 0.0).astype(BF16)
        earlier = dot(member.astype(BF16), before)
        code = jnp.where(member > 0.5, earlier, 9.0)
        r.info_out[...] = jnp.full(r.info_out.shape, 9.0, F32)
        for q in range(nk):
            r.info_out[q, 0:nz, 0:seqs] = code[q * nz : (q + 1) * nz]
            r.info_out[q, nz : 2 * nz, 0:seqs] = weight[q * nz : (q + 1) * nz]
        r.resid[:, seqs:, :] = jnp.zeros((nk, LANES - seqs, width), BF16)
        r.up_vm[0:low, wide:] = jnp.zeros((low, wide), BF16)
        r.up_vm[low:, 0:wide] = jnp.zeros((low, wide), BF16)

    with scope("project"):
        settle(r.tokens_vm, load_sem["tokens"])
        normed = row_norm(r.tokens_vm[...].astype(F32)).astype(BF16)
        settle(r.low_vm, load_sem["low"])
        lowered = dot_last(normed, r.low_vm[...])
        lane = lax.broadcasted_iota(I32, (seqs, 2 * low), 1)
        lowered = jnp.where(lane < low, jnp.tanh(lowered), lowered).astype(BF16)
        settle(r.qkv_vm, load_sem["qkv"])
        qkv = dot(normed, r.qkv_vm[...]).astype(BF16).astype(F32)
        recept, keys, values = qkv[:, :wide], qkv[:, wide : 2 * wide], qkv[:, 2 * wide :]
        settle(r.up_vm.at[pl.ds(0, low)], load_sem["up"])
        for ref in (r.base_vm, r.rate_vm, r.gain_vm):
            settle(ref, load_sem["rows"])
        raised = dot(lowered, r.up_vm[...])
        decay = jnp.exp(
            -jax.nn.sigmoid(raised[:, :wide] + r.base_vm[...]) * 0.6065306597126334
        )
        rate = jax.nn.sigmoid(raised[:, wide:] + r.rate_vm[...])

    lane = lax.broadcasted_iota(I32, (seqs, wide), 1)

    def head_sum(operand):
        total = jnp.zeros((seqs, wide), F32)
        for h in range(heads):
            mine = lane // head == h
            part = jnp.sum(jnp.where(mine, operand, 0.0), axis=1, keepdims=True)
            total = jnp.where(mine, part, total)
        return total

    with scope("heads"):
        unit = keys * lax.rsqrt(head_sum(keys * keys) + UNIT_EPS)
        unit_rate, key_rate = unit * rate, keys * rate

        def first_lanes(operand, h):
            return pltpu.roll(operand, wide - head * h, 1) if h else operand

        for h in range(heads):
            r.vec_vm[3 * h] = first_lanes(decay, h)
            r.vec_vm[3 * h + 1] = first_lanes(unit_rate, h)
            r.vec_vm[3 * h + 2] = first_lanes(key_rate, h)
        probes = [first_lanes(unit, h)[:, :head] for h in range(heads)]
        decayed = decay * recept
        probes += [first_lanes(decayed, h)[:, :head] for h in range(heads)]
        row8 = lax.broadcasted_iota(I32, (8, wide), 0)
        lane8 = lax.broadcasted_iota(I32, (8, wide), 1)
        found = [[], []]
        for s in range(0, seqs, 8):
            settle(r.new_state.at[pl.ds(s, 8)], load_sem[s])
            left = jnp.concatenate([probe[s : s + 8] for probe in probes], axis=0).astype(BF16)
            right = r.new_state[s : s + 8].reshape(8 * wide, head).astype(BF16)
            product = dot_last(left, right)
            for what in range(2):
                total = jnp.zeros((8, wide), F32)
                for h in range(heads):
                    at = (what * heads + h) * 8
                    for i in range(8):
                        here = jnp.logical_and(row8 == i, lane8 // head == h)
                        total = jnp.where(
                            here, product[at : at + 8, i * wide : (i + 1) * wide], total
                        )
                found[what].append(total)
        state_unit = jnp.concatenate(found[0], axis=0)
        head_out = (
            jnp.concatenate(found[1], axis=0)
            - state_unit * head_sum(unit_rate * recept)
            + values * head_sum(key_rate * recept)
        )
        r.col_vm[0] = state_unit
        r.col_vm[1] = values
        centred = head_out - head_sum(head_out) * (1.0 / head)
        spread = head_sum(centred * centred) * (1.0 / head)
        mixed = (centred * lax.rsqrt(spread + GROUP_EPS) * r.gain_vm[...]).astype(BF16)
        settle(r.out_vm, load_sem["out"])
        partial = dot(mixed, r.out_vm[...])
        for q in range(ny):
            r.part_out[q] = partial[:, q * width : (q + 1) * width].astype(BF16)

    with scope("barrier"):
        pl.semaphore_wait(barrier, len(peers))

    for q in lanes:
        send(
            r.part_out.at[(y + q) % ny],
            r.part_in.at[q],
            r.part_send.at[0],
            r.part_recv.at[0],
            in_y(q),
        )
    for q in others:
        send(r.info_out.at[q], r.info_in.at[q], r.info_send.at[0], r.info_recv.at[0], in_plane(q))

    with scope("reduce"):
        summed = r.part_out[y].astype(F32)
        settle(r.part_in.at[pl.ds(1, ny - 1)], r.part_recv.at[0])
        for q in range(1, ny):
            summed = summed + r.part_in[q].astype(F32)
        own = r.tokens_vm[:, pl.ds(pl.multiple_of(y * width, LANES), width)]
        r.resid[0, 0:seqs, :] = (own.astype(F32) + summed).astype(BF16)
    for q in others:
        send(
            r.resid.at[0, pl.ds(0, seqs)],
            r.resid.at[q, pl.ds(0, seqs)],
            r.res_send.at[0],
            r.res_recv.at[0],
            in_plane(q),
        )

    with scope("pick"):
        rep_row = lax.broadcasted_iota(I32, (nz, SLOTS, nk, nz), 0).reshape(rows, nz)
        rep_col = lax.broadcasted_iota(I32, (nz, SLOTS, nk, nz), 3).reshape(rows, nz)
        repeat = jnp.where(rep_row == rep_col, 1.0, 0.0).astype(BF16)
        slot = lax.broadcasted_iota(I32, (nz, SLOTS, nk, LANES), 1).reshape(rows, LANES).astype(F32)
        source = lax.broadcasted_iota(I32, (nz, SLOTS, nk, LANES), 2).reshape(rows, LANES)
        settle(r.info_in.at[pl.ds(1, nk - 1)], r.info_recv.at[0])
        for q in range(nk):
            told = r.info_in if q else r.info_out
            spread = dot(repeat, told[q, 0:nz, :].astype(BF16))
            chosen = jnp.where(spread == slot, jnp.where(source == q, 1.0, 0.0), 0.0)
            r.pick[:, q * LANES : (q + 1) * LANES] = chosen.astype(BF16)

    with scope("gather"):
        settle(r.resid.at[pl.ds(1, nk - 1), pl.ds(0, seqs)], r.res_recv.at[0])
    with scope("dispatch"):
        outgoing = dot(r.pick[...], r.resid[...].reshape(nk * LANES, width))
        outgoing = outgoing.reshape(nz, block, width)
        r.z_out[...] = jnp.concatenate(
            [outgoing[:, :, :half], outgoing[:, :, half:]], axis=1
        ).astype(BF16)

    for j in send_order(nz):
        send(r.z_out.at[j], r.z_in.at[j], r.z_send.at[0], r.z_recv.at[j], in_z(j))

    def forward(source, group):
        span = pl.ds(group[0], len(group))
        for q in lanes:
            target = r.y_in.at[q, span]
            send(source.at[span], target, r.y_send.at[0], r.y_recv.at[group_of[group[0]]], in_y(q))

    def forward_group(group):
        group = [j for j in group if j]
        for j in group:
            settle(r.z_in.at[j], r.z_recv.at[j])
        if group:
            forward(r.z_in, group)

    forward(r.z_out, [0])

    def experts(group):
        at = (pl.ds(1, ny - 1), pl.ds(group[0], len(group)))
        settle(r.y_in.at[at], r.y_recv.at[group_of[group[0]]])
        columns = []
        for q in range(ny):
            pieces = []
            for j in group:
                if q:
                    held = r.y_in[q, j]
                elif j:
                    held = r.z_in[j]
                else:
                    held = r.z_out[0]
                held = held.astype(F32)
                pieces.append(jnp.concatenate([held[:block], held[block:]], axis=1))
            columns.append(jnp.concatenate(pieces, axis=0))
        features = jnp.concatenate(columns, axis=1)
        normed = row_norm(features).astype(BF16)
        pre = dot(normed, r.gu_vm[...])
        gated = jnp.minimum(pre[:, :hidden], CLAMP_LIMIT)
        linear = jnp.clip(pre[:, hidden:], -CLAMP_LIMIT, CLAMP_LIMIT)
        activated = (gated * jax.nn.sigmoid(GLU_ALPHA * gated) * (linear + 1.0)).astype(BF16)
        share = dot(activated, r.down_vm[...])
        for q in range(ny):
            for at, j in enumerate(group):
                piece = share[at * block : (at + 1) * block, q * width : (q + 1) * width]
                r.share_out[q, j] = jnp.concatenate(
                    [piece[:, :half], piece[:, half:]], axis=0
                ).astype(BF16)
        for q in lanes:
            at = (q, pl.ds(group[0], len(group)))
            g = group_of[group[0]]
            send(
                r.share_out.at[at], r.share_in.at[at], r.share_send.at[0], r.share_recv.at[g], in_y(q)
            )

    def give_back(group):
        at = (pl.ds(1, ny - 1), pl.ds(group[0], len(group)))
        settle(r.share_in.at[at], r.share_recv.at[group_of[group[0]]])
        for j in group:
            total = r.share_out[0, j].astype(F32)
            for q in range(1, ny):
                total = total + r.share_in[q, j].astype(F32)
            total = total.astype(BF16)
            if j:
                r.back_out[j] = total
                send(
                    r.back_out.at[j], r.back_in.at[j], r.back_send.at[0], r.back_recv.at[0], out_z(j)
                )
            else:
                r.back_in[0] = total

    def return_weights():
        for q in range(nk):
            told = r.info_in if q else r.info_out
            weight = told[q, nz : 2 * nz, :]
            high = weight.astype(BF16)
            low_part = (weight - high.astype(F32)).astype(BF16)
            spread = dot(repeat, high) + dot(repeat, low_part)
            scaled = (spread * r.pick[:, q * LANES : (q + 1) * LANES].astype(F32)).T[0:seqs, :]
            high = scaled.astype(BF16)
            r.mix_hi[q] = high
            r.mix_lo[q] = (scaled - high.astype(F32)).astype(BF16)

    for step in plan(len(groups)):
        with scope(step):
            if step == "L":
                settle(r.gu_vm, load_sem["gu"])
                settle(r.down_vm, load_sem["down"])
            elif step == "W":
                return_weights()
            else:
                work = dict(F=forward_group, E=experts, B=give_back)[step[0]]
                work(groups[int(step[1:])])
    with scope("state"):
        for s in range(0, seqs, 8):
            lost = r.col_vm[0, s : s + 8, :].T
            gained = r.col_vm[1, s : s + 8, :].T
            for i in range(8):
                for h in range(heads):
                    at = pl.ds(s + i, 1)
                    span = slice(h * head, (h + 1) * head)
                    r.new_state[s + i, h] = (
                        r.new_state[s + i, h] * r.vec_vm[3 * h, at, :][:, :head]
                        - lost[span, i : i + 1] * r.vec_vm[3 * h + 1, at, :][:, :head]
                        + gained[span, i : i + 1] * r.vec_vm[3 * h + 2, at, :][:, :head]
                    )

    with scope("returned"):
        settle(r.back_in.at[pl.ds(1, nz - 1)], r.back_recv.at[0])
    with scope("mix"):
        returned = r.back_in[...].astype(F32)
        returned = jnp.concatenate([returned[:, :block], returned[:, block:]], axis=2)
        returned = returned.reshape(rows, width).astype(BF16)
        mixture = dot(r.mix_hi[...].reshape(nk * seqs, rows), returned) + dot(
            r.mix_lo[...].reshape(nk * seqs, rows), returned
        )
        r.mix_out[...] = mixture.reshape(nk, seqs, width).astype(BF16)
    for q in others:
        send(r.mix_out.at[q], r.mix_in.at[q], r.mix_send.at[0], r.mix_recv.at[0], back_plane(q))
    with scope("final"):
        total = mixture[0:seqs]
        settle(r.mix_in.at[pl.ds(1, nk - 1)], r.mix_recv.at[0])
        for q in range(1, nk):
            total = total + r.mix_in[q].astype(F32)
        r.layer_out[...] = (r.resid[0, 0:seqs, :].astype(F32) + total).astype(BF16)
    with scope("drain"):
        settle(r.part_in.at[pl.ds(1, ny - 1)], r.part_send.at[0])
        settle(r.info_in.at[pl.ds(1, nk - 1)], r.info_send.at[0])
        settle(r.resid.at[pl.ds(1, nk - 1), pl.ds(0, seqs)], r.res_send.at[0])
        settle(r.z_in.at[pl.ds(1, nz - 1)], r.z_send.at[0])
        settle(r.y_in.at[pl.ds(1, ny - 1)], r.y_send.at[0])
        settle(r.share_in.at[pl.ds(1, ny - 1)], r.share_send.at[0])
        settle(r.back_in.at[pl.ds(1, nz - 1)], r.back_send.at[0])
        settle(r.mix_in.at[pl.ds(1, nk - 1)], r.mix_send.at[0])


def run_layer(sizes, *operands):
    nz, nk, ny, seqs, width = sizes
    args = dict(zip(INPUTS, operands, strict=True))
    rows = nz * SLOTS * nk
    message = (2 * SLOTS * nk, width // 2)
    hidden = args["gate"].shape[2]
    wide = args["recept"].shape[1]
    low = args["decay_down"].shape[0]
    state = args["state"].shape
    heads = state[1]
    dma = pltpu.SemaphoreType.DMA
    scratch = dict(
        tokens_vm=pltpu.VMEM((seqs, ny * width), BF16),
        qkv_vm=pltpu.VMEM((ny * width, 3 * wide), BF16),
        low_vm=pltpu.VMEM((2 * low, ny * width), BF16),
        up_vm=pltpu.VMEM((2 * low, 2 * wide), BF16),
        base_vm=pltpu.VMEM((1, wide), F32),
        rate_vm=pltpu.VMEM((1, wide), F32),
        gain_vm=pltpu.VMEM((1, wide), F32),
        routes_vm=pltpu.VMEM(args["routes"].shape, I32),
        weights_vm=pltpu.VMEM(args["weights"].shape, F32),
        vec_vm=pltpu.VMEM((3 * heads, seqs, wide), F32),
        col_vm=pltpu.VMEM((2, seqs, wide), F32),
        out_vm=pltpu.VMEM((wide, ny * width), BF16),
        gu_vm=pltpu.VMEM((ny * width, 2 * hidden), BF16),
        down_vm=pltpu.VMEM((hidden, ny * width), BF16),
        info_out=pltpu.VMEM((nk, 2 * nz, LANES), F32),
        info_in=pltpu.VMEM((nk, 2 * nz, LANES), F32),
        part_out=pltpu.VMEM((ny, seqs, width), BF16),
        part_in=pltpu.VMEM((ny, seqs, width), BF16),
        resid=pltpu.VMEM((nk, LANES, width), BF16),
        pick=pltpu.VMEM((rows, nk * LANES), BF16),
        mix_hi=pltpu.VMEM((nk, seqs, rows), BF16),
        mix_lo=pltpu.VMEM((nk, seqs, rows), BF16),
        z_out=pltpu.VMEM((nz, *message), BF16),
        z_in=pltpu.VMEM((nz, *message), BF16),
        y_in=pltpu.VMEM((ny, nz, *message), BF16),
        share_out=pltpu.VMEM((ny, nz, *message), BF16),
        share_in=pltpu.VMEM((ny, nz, *message), BF16),
        back_out=pltpu.VMEM((nz, *message), BF16),
        back_in=pltpu.VMEM((nz, *message), BF16),
        mix_out=pltpu.VMEM((nk, seqs, width), BF16),
        mix_in=pltpu.VMEM((nk, seqs, width), BF16),
        load_sem=dma((9 + seqs // 8,)),
    )
    waits = len(plane_groups(nz))
    for name, count in dict(
        info=1, part=1, res=1, z=nz, y=waits, share=waits, back=1, mix=1
    ).items():
        scratch[name + "_send"] = dma((1,))
        scratch[name + "_recv"] = dma((count,))
    hbm = pl.BlockSpec(memory_space=pltpu.HBM)
    vmem = pl.BlockSpec(memory_space=pltpu.VMEM)
    names = INPUTS + ["layer_out", "new_state"] + list(scratch)
    outs = ((seqs, width), BF16), (state, F32)
    results = pl.pallas_call(
        functools.partial(layer_kernel, sizes, names),
        out_shape=tuple(pltpu.VMEM(*out) for out in outs),
        in_specs=[hbm] * len(INPUTS),
        out_specs=(vmem, vmem),
        scratch_shapes=list(scratch.values()),
        compiler_params=pltpu.CompilerParams(
            collective_id=0, has_side_effects=True, vmem_limit_bytes=60 * 1024 * 1024
        ),
        name="layer",
    )(*operands)
    return pl.pallas_call(
        store_kernel,
        out_shape=tuple(jax.ShapeDtypeStruct(*out) for out in outs),
        in_specs=[vmem, vmem],
        out_specs=(hbm, hbm),
        scratch_shapes=[dma((PIECES + 1,))],
        compiler_params=pltpu.CompilerParams(vmem_limit_bytes=1024 * 1024),
        name="store",
    )(*results)


def store_kernel(layer_vm, state_vm, layer_ref, state_ref, sems):
    size = state_vm.shape[0] // PIECES
    copies = [pltpu.make_async_copy(layer_vm, layer_ref, sems.at[PIECES])]
    for i in range(PIECES):
        at = pl.ds(i * size, size)
        copies.append(pltpu.make_async_copy(state_vm.at[at], state_ref.at[at], sems.at[i]))
    for copy in copies:
        copy.start()
    for copy in copies:
        copy.wait()


def local(
    tokens,
    head_state,
    recept_weight,
    key_weight,
    value_weight,
    decay_down_factor,
    decay_up_factor,
    decay_base,
    rate_down_factor,
    rate_up_factor,
    rate_base,
    head_gain,
    out_weight,
    route_experts,
    route_weights,
    expert_gate,
    expert_up,
    expert_down,
):
    ny = lax.axis_size("tp")
    nz = lax.axis_size("ep") // PLANE
    seqs, model = tokens.shape

    return run_layer(
        (nz, PLANE, ny, seqs, model // ny),
        tokens,
        head_state,
        recept_weight,
        key_weight,
        value_weight,
        decay_down_factor.T,
        decay_up_factor,
        decay_base[None],
        rate_down_factor.T,
        rate_up_factor,
        rate_base[None],
        head_gain[None],
        out_weight,
        route_experts.T,
        route_weights.T,
        expert_gate,
        expert_up,
        expert_down,
    )


def solution(mesh):
    in_specs = (
        P("ep", None),
        P("ep", "tp", None, None),
        P(None, "tp"),
        P(None, "tp"),
        P(None, "tp"),
        P(),
        P(None, "tp"),
        P("tp"),
        P(),
        P(None, "tp"),
        P("tp"),
        P("tp"),
        P("tp", None),
        P("ep", None),
        P("ep", None),
        P("ep", None, "tp"),
        P("ep", None, "tp"),
        P("ep", "tp", None),
    )
    out_specs = (P("ep", "tp"), P("ep", "tp", None, None))
    return jax.shard_map(local, mesh=mesh, in_specs=in_specs, out_specs=out_specs, check_vma=False)
```

```python
import contextlib
import functools
import types

import jax
import jax.numpy as jnp
from jax import lax
from jax.experimental import pallas as pl
from jax.experimental.pallas import tpu as pltpu
from jax.sharding import PartitionSpec as P

NORM_EPS = 1e-05
GROUP_EPS = 0.00064
UNIT_EPS = 1e-06
CLAMP_LIMIT = 7.0
GLU_ALPHA = 1.702
PLANE = 8
SLOTS = 3
LANES = 128
WORK_ORDER = [0, 1, 2, 8, 7, 6, 5, 4, 3]
SEND_ORDER = [1, 2, 8, 7, 6, 5, 4, 3]
CUTS = [0, 3, 5, 9, 13, 16]
PLAN = ["F0", "L", "F1", "W", "E0", "E1", "F2", "F3", "F4", "B0", "B1", "E2", "E3", "E4", "B2", "B3", "B4"]
PIECES = 6
SCOPES = False
MESH = pl.DeviceIdType.MESH
F32, BF16, I32 = jnp.float32, jnp.bfloat16, jnp.int32


def plane_offsets(nz):
    if nz == 2 * len(WORK_ORDER) - 2:
        half = [way * d for d in WORK_ORDER for way in ((1, -1) if 0 < d < nz // 2 else (1,))]
        return half
    return [0] + [way * d for d in range(1, nz // 2) for way in (1, -1)] + [nz // 2]


def send_order(nz):
    offsets = plane_offsets(nz)
    if nz == 2 * len(SEND_ORDER):
        return [j for d in SEND_ORDER for j in range(nz) if abs(offsets[j]) == d]
    return list(range(1, nz))


def plane_groups(nz):
    cuts = CUTS if nz == 16 else [0, nz // 2, nz]
    return [range(low, high) for low, high in zip(cuts, cuts[1:])]


def plan(count):
    if count == len(CUTS) - 1:
        return PLAN
    steps = ["F0", "L"] + [f"F{g}" for g in range(1, count)] + [f"E{g}" for g in range(count)]
    return steps + [f"B{g}" for g in range(count)] + ["W"]


def scope(name):
    return jax.named_scope(name) if SCOPES else contextlib.nullcontext()


def row_norm(values):
    return values * lax.rsqrt(jnp.mean(values * values, axis=-1, keepdims=True) + NORM_EPS)


def dot(a, b):
    return jnp.dot(a, b, preferred_element_type=F32)


def dot_last(a, b):
    return lax.dot_general(a, b, (((1,), (1,)), ((), ())), preferred_element_type=F32)


INPUTS = [
    "tokens",
    "state",
    "recept",
    "key",
    "value",
    "decay_down",
    "decay_up",
    "decay_base",
    "rate_down",
    "rate_up",
    "rate_base",
    "gain",
    "out_weight",
    "routes",
    "weights",
    "gate",
    "up",
    "down",
]


def layer_kernel(sizes, names, *refs):
    nz, nk, ny, seqs, width = sizes
    r = types.SimpleNamespace(**dict(zip(names, refs, strict=True)))
    half = width // 2
    block = SLOTS * nk
    rows = nz * block
    groups = plane_groups(nz)
    group_of = {j: g for g, group in enumerate(groups) for j in group}
    ep = lax.axis_index("ep")
    y = lax.axis_index("tp")
    z, k = ep // nk, ep % nk

    offsets = [offset % nz for offset in plane_offsets(nz)]

    def in_z(j):
        return ((z + offsets[j]) % nz) * nk + k, y

    def out_z(j):
        return ((z + (nz - offsets[j])) % nz) * nk + k, y

    def in_plane(q):
        return z * nk + (k + q) % nk, y

    def back_plane(q):
        return z * nk + (k + (nk - q)) % nk, y

    def in_y(q):
        return ep, (y + q) % ny

    lanes = sorted(range(1, ny), key=lambda q: -min(q, ny - q))
    others = sorted(range(1, nk), key=lambda q: -min(q, nk - q))

    def send(source, target, sends, receives, device):
        pltpu.make_async_remote_copy(
            src_ref=source,
            dst_ref=target,
            send_sem=sends,
            recv_sem=receives,
            device_id=device,
            device_id_type=MESH,
        ).start()

    def settle(ref, sem):
        pltpu.make_async_copy(ref, ref, sem).wait()

    barrier = pltpu.get_barrier_semaphore()
    peers = (
        [in_z(j) for j in range(nz - 1, 0, -1)]
        + [in_plane(q) for q in range(1, nk)]
        + [in_y(q) for q in range(1, ny)]
    )
    for device in peers:
        pl.semaphore_signal(barrier, inc=1, device_id=device, device_id_type=MESH)

    order = ["tokens", "low", "qkv", "up", "rows", "out", "gu", "down", "routes"]
    load_sem = {name: r.load_sem.at[i] for i, name in enumerate(order)}
    for s in range(0, seqs, 8):
        load_sem[s] = r.load_sem.at[len(order) + s // 8]

    def load(name, source, target):
        pltpu.make_async_copy(source, target, load_sem[name]).start()

    wide = r.recept.shape[1]
    low = r.decay_down.shape[0]
    heads = r.state.shape[1]
    head = wide // heads
    load("routes", r.routes, r.routes_vm)
    load("routes", r.weights, r.weights_vm)
    load("tokens", r.tokens, r.tokens_vm)
    load("low", r.decay_down, r.low_vm.at[pl.ds(0, low)])
    load("low", r.rate_down, r.low_vm.at[pl.ds(low, low)])
    load("qkv", r.recept, r.qkv_vm.at[:, pl.ds(0, wide)])
    load("qkv", r.key, r.qkv_vm.at[:, pl.ds(wide, wide)])
    load("qkv", r.value, r.qkv_vm.at[:, pl.ds(2 * wide, wide)])
    load("up", r.decay_up, r.up_vm.at[pl.ds(0, low), pl.ds(0, wide)])
    load("up", r.rate_up, r.up_vm.at[pl.ds(low, low), pl.ds(wide, wide)])
    load("rows", r.decay_base, r.base_vm)
    load("rows", r.rate_base, r.rate_vm)
    load("rows", r.gain, r.gain_vm)
    for s in range(0, seqs, 8):
        load(s, r.state.at[pl.ds(s, 8)], r.new_state.at[pl.ds(s, 8)])
    load("out", r.out_weight, r.out_vm)
    hidden = r.gate.shape[2]
    for q in range(ny):
        own = pl.ds(pl.multiple_of(((y + (ny - q)) % ny) * width, LANES), width)
        put = pl.ds(q * width, width)
        load("gu", r.gate.at[0, own, :], r.gu_vm.at[put, pl.ds(0, hidden)])
        load("gu", r.up.at[0, own, :], r.gu_vm.at[put, pl.ds(hidden, hidden)])
    for q in range(ny):
        ahead = pl.ds(pl.multiple_of(((y + q) % ny) * width, LANES), width)
        load("down", r.down.at[0, :, ahead], r.down_vm.at[:, pl.ds(q * width, width)])

    with scope("tables"):
        count = nk * nz
        row = lax.broadcasted_iota(I32, (count, seqs), 0)
        j_of, q_of = row % nz, row // nz
        away = jnp.zeros((count, seqs), I32)
        for j, offset in enumerate(offsets):
            away = jnp.where(j_of == j, offset, away)
        expert = ((z + away) % nz) * nk + (k + q_of) % nk
        member = jnp.zeros((count, seqs), F32)
        weight = jnp.zeros((count, seqs), F32)
        settle(r.routes_vm, load_sem["routes"])
        settle(r.weights_vm, load_sem["routes"])
        for c in range(r.routes.shape[0]):
            named = r.routes_vm[c : c + 1, :] == expert
            member = member + jnp.where(named, 1.0, 0.0)
            weight = weight + jnp.where(named, r.weights_vm[c : c + 1, :], 0.0)
        earlier_row = lax.broadcasted_iota(I32, (seqs, seqs), 0)
        later_row = lax.broadcasted_iota(I32, (seqs, seqs), 1)
        before = jnp.where(earlier_row < later_row, 1.0, 0.0).astype(BF16)
        earlier = dot(member.astype(BF16), before)
        code = jnp.where(member > 0.5, earlier, 9.0)
        r.info_out[...] = jnp.full(r.info_out.shape, 9.0, F32)
        for q in range(nk):
            r.info_out[q, 0:nz, 0:seqs] = code[q * nz : (q + 1) * nz]
            r.info_out[q, nz : 2 * nz, 0:seqs] = weight[q * nz : (q + 1) * nz]
        r.resid[:, seqs:, :] = jnp.zeros((nk, LANES - seqs, width), BF16)
        r.up_vm[0:low, wide:] = jnp.zeros((low, wide), BF16)
        r.up_vm[low:, 0:wide] = jnp.zeros((low, wide), BF16)

    with scope("project"):
        settle(r.tokens_vm, load_sem["tokens"])
        normed = row_norm(r.tokens_vm[...].astype(F32)).astype(BF16)
        settle(r.low_vm, load_sem["low"])
        lowered = dot_last(normed, r.low_vm[...])
        lane = lax.broadcasted_iota(I32, (seqs, 2 * low), 1)
        lowered = jnp.where(lane < low, jnp.tanh(lowered), lowered).astype(BF16)
        settle(r.qkv_vm, load_sem["qkv"])
        qkv = dot(normed, r.qkv_vm[...]).astype(BF16).astype(F32)
        recept, keys, values = qkv[:, :wide], qkv[:, wide : 2 * wide], qkv[:, 2 * wide :]
        settle(r.up_vm.at[pl.ds(0, low)], load_sem["up"])
        for ref in (r.base_vm, r.rate_vm, r.gain_vm):
            settle(ref, load_sem["rows"])
        raised = dot(lowered, r.up_vm[...])
        decay = jnp.exp(
            -jax.nn.sigmoid(raised[:, :wide] + r.base_vm[...]) * 0.6065306597126334
        )
        rate = jax.nn.sigmoid(raised[:, wide:] + r.rate_vm[...])

    lane = lax.broadcasted_iota(I32, (seqs, wide), 1)

    def head_sum(operand):
        total = jnp.zeros((seqs, wide), F32)
        for h in range(heads):
            mine = lane // head == h
            part = jnp.sum(jnp.where(mine, operand, 0.0), axis=1, keepdims=True)
            total = jnp.where(mine, part, total)
        return total

    with scope("heads"):
        unit = keys * lax.rsqrt(head_sum(keys * keys) + UNIT_EPS)
        unit_rate, key_rate = unit * rate, keys * rate

        def first_lanes(operand, h):
            return pltpu.roll(operand, wide - head * h, 1) if h else operand

        for h in range(heads):
            r.vec_vm[3 * h] = first_lanes(decay, h)
            r.vec_vm[3 * h + 1] = first_lanes(unit_rate, h)
            r.vec_vm[3 * h + 2] = first_lanes(key_rate, h)
        probes = [first_lanes(unit, h)[:, :head] for h in range(heads)]
        decayed = decay * recept
        probes += [first_lanes(decayed, h)[:, :head] for h in range(heads)]
        row8 = lax.broadcasted_iota(I32, (8, wide), 0)
        lane8 = lax.broadcasted_iota(I32, (8, wide), 1)
        found = [[], []]
        for s in range(0, seqs, 8):
            settle(r.new_state.at[pl.ds(s, 8)], load_sem[s])
            left = jnp.concatenate([probe[s : s + 8] for probe in probes], axis=0).astype(BF16)
            right = r.new_state[s : s + 8].reshape(8 * wide, head).astype(BF16)
            product = dot_last(left, right)
            for what in range(2):
                total = jnp.zeros((8, wide), F32)
                for h in range(heads):
                    at = (what * heads + h) * 8
                    for i in range(8):
                        here = jnp.logical_and(row8 == i, lane8 // head == h)
                        total = jnp.where(
                            here, product[at : at + 8, i * wide : (i + 1) * wide], total
                        )
                found[what].append(total)
        state_unit = jnp.concatenate(found[0], axis=0)
        head_out = (
            jnp.concatenate(found[1], axis=0)
            - state_unit * head_sum(unit_rate * recept)
            + values * head_sum(key_rate * recept)
        )
        r.col_vm[0] = state_unit
        r.col_vm[1] = values
        centred = head_out - head_sum(head_out) * (1.0 / head)
        spread = head_sum(centred * centred) * (1.0 / head)
        mixed = (centred * lax.rsqrt(spread + GROUP_EPS) * r.gain_vm[...]).astype(BF16)
        settle(r.out_vm, load_sem["out"])
        partial = dot(mixed, r.out_vm[...])
        for q in range(ny):
            r.part_out[q] = partial[:, q * width : (q + 1) * width].astype(BF16)

    with scope("barrier"):
        pl.semaphore_wait(barrier, len(peers))

    for q in lanes:
        send(
            r.part_out.at[(y + q) % ny],
            r.part_in.at[q],
            r.part_send.at[0],
            r.part_recv.at[0],
            in_y(q),
        )
    for q in others:
        send(r.info_out.at[q], r.info_in.at[q], r.info_send.at[0], r.info_recv.at[0], in_plane(q))

    with scope("reduce"):
        summed = r.part_out[y].astype(F32)
        settle(r.part_in.at[pl.ds(1, ny - 1)], r.part_recv.at[0])
        for q in range(1, ny):
            summed = summed + r.part_in[q].astype(F32)
        own = r.tokens_vm[:, pl.ds(pl.multiple_of(y * width, LANES), width)]
        r.resid[0, 0:seqs, :] = (own.astype(F32) + summed).astype(BF16)
    for q in others:
        send(
            r.resid.at[0, pl.ds(0, seqs)],
            r.resid.at[q, pl.ds(0, seqs)],
            r.res_send.at[0],
            r.res_recv.at[0],
            in_plane(q),
        )

    with scope("pick"):
        rep_row = lax.broadcasted_iota(I32, (nz, SLOTS, nk, nz), 0).reshape(rows, nz)
        rep_col = lax.broadcasted_iota(I32, (nz, SLOTS, nk, nz), 3).reshape(rows, nz)
        repeat = jnp.where(rep_row == rep_col, 1.0, 0.0).astype(BF16)
        slot = lax.broadcasted_iota(I32, (nz, SLOTS, nk, LANES), 1).reshape(rows, LANES).astype(F32)
        source = lax.broadcasted_iota(I32, (nz, SLOTS, nk, LANES), 2).reshape(rows, LANES)
        settle(r.info_in.at[pl.ds(1, nk - 1)], r.info_recv.at[0])
        for q in range(nk):
            told = r.info_in if q else r.info_out
            spread = dot(repeat, told[q, 0:nz, :].astype(BF16))
            chosen = jnp.where(spread == slot, jnp.where(source == q, 1.0, 0.0), 0.0)
            r.pick[:, q * LANES : (q + 1) * LANES] = chosen.astype(BF16)

    with scope("gather"):
        settle(r.resid.at[pl.ds(1, nk - 1), pl.ds(0, seqs)], r.res_recv.at[0])
    def dispatch(low, high):
        outgoing = dot(
            r.pick[low * block : high * block, :], r.resid[...].reshape(nk * LANES, width)
        ).reshape(high - low, block, width)
        r.z_out[low:high] = jnp.concatenate(
            [outgoing[:, :, :half], outgoing[:, :, half:]], axis=1
        ).astype(BF16)
        for j in send_order(nz):
            if low <= j < high:
                send(r.z_out.at[j], r.z_in.at[j], r.z_send.at[0], r.z_recv.at[j], in_z(j))

    with scope("dispatch"):
        cut = 6 if nz == 16 else nz // 2
        dispatch(0, cut)
        dispatch(cut, nz)

    def forward(source, group):
        span = pl.ds(group[0], len(group))
        for q in lanes:
            target = r.y_in.at[q, span]
            send(source.at[span], target, r.y_send.at[0], r.y_recv.at[group_of[group[0]]], in_y(q))

    def forward_group(group):
        group = [j for j in group if j]
        for j in group:
            settle(r.z_in.at[j], r.z_recv.at[j])
        if group:
            forward(r.z_in, group)

    forward(r.z_out, [0])

    def experts(group):
        at = (pl.ds(1, ny - 1), pl.ds(group[0], len(group)))
        settle(r.y_in.at[at], r.y_recv.at[group_of[group[0]]])
        columns = []
        for q in range(ny):
            pieces = []
            for j in group:
                if q:
                    held = r.y_in[q, j]
                elif j:
                    held = r.z_in[j]
                else:
                    held = r.z_out[0]
                held = held.astype(F32)
                pieces.append(jnp.concatenate([held[:block], held[block:]], axis=1))
            columns.append(jnp.concatenate(pieces, axis=0))
        features = jnp.concatenate(columns, axis=1)
        normed = row_norm(features).astype(BF16)
        pre = dot(normed, r.gu_vm[...])
        gated = jnp.minimum(pre[:, :hidden], CLAMP_LIMIT)
        linear = jnp.clip(pre[:, hidden:], -CLAMP_LIMIT, CLAMP_LIMIT)
        activated = (gated * jax.nn.sigmoid(GLU_ALPHA * gated) * (linear + 1.0)).astype(BF16)
        share = dot(activated, r.down_vm[...])
        for q in range(ny):
            for at, j in enumerate(group):
                piece = share[at * block : (at + 1) * block, q * width : (q + 1) * width]
                r.share_out[q, j] = jnp.concatenate(
                    [piece[:, :half], piece[:, half:]], axis=0
                ).astype(BF16)
        for q in lanes:
            at = (q, pl.ds(group[0], len(group)))
            g = group_of[group[0]]
            send(
                r.share_out.at[at], r.share_in.at[at], r.share_send.at[0], r.share_recv.at[g], in_y(q)
            )

    def give_back(group):
        at = (pl.ds(1, ny - 1), pl.ds(group[0], len(group)))
        settle(r.share_in.at[at], r.share_recv.at[group_of[group[0]]])
        for j in group:
            total = r.share_out[0, j].astype(F32)
            for q in range(1, ny):
                total = total + r.share_in[q, j].astype(F32)
            total = total.astype(BF16)
            if j:
                r.back_out[j] = total
                send(
                    r.back_out.at[j], r.back_in.at[j], r.back_send.at[0], r.back_recv.at[0], out_z(j)
                )
            else:
                r.back_in[0] = total

    def return_weights():
        for q in range(nk):
            told = r.info_in if q else r.info_out
            weight = told[q, nz : 2 * nz, :]
            high = weight.astype(BF16)
            low_part = (weight - high.astype(F32)).astype(BF16)
            spread = dot(repeat, high) + dot(repeat, low_part)
            scaled = (spread * r.pick[:, q * LANES : (q + 1) * LANES].astype(F32)).T[0:seqs, :]
            high = scaled.astype(BF16)
            r.mix_hi[q] = high
            r.mix_lo[q] = (scaled - high.astype(F32)).astype(BF16)

    for step in plan(len(groups)):
        with scope(step):
            if step == "L":
                settle(r.gu_vm, load_sem["gu"])
                settle(r.down_vm, load_sem["down"])
            elif step == "W":
                return_weights()
            else:
                work = dict(F=forward_group, E=experts, B=give_back)[step[0]]
                work(groups[int(step[1:])])
    with scope("state"):
        for s in range(0, seqs, 8):
            lost = r.col_vm[0, s : s + 8, :].T
            gained = r.col_vm[1, s : s + 8, :].T
            for i in range(8):
                for h in range(heads):
                    at = pl.ds(s + i, 1)
                    span = slice(h * head, (h + 1) * head)
                    r.new_state[s + i, h] = (
                        r.new_state[s + i, h] * r.vec_vm[3 * h, at, :][:, :head]
                        - lost[span, i : i + 1] * r.vec_vm[3 * h + 1, at, :][:, :head]
                        + gained[span, i : i + 1] * r.vec_vm[3 * h + 2, at, :][:, :head]
                    )

    with scope("returned"):
        settle(r.back_in.at[pl.ds(1, nz - 1)], r.back_recv.at[0])
    with scope("mix"):
        returned = r.back_in[...].astype(F32)
        returned = jnp.concatenate([returned[:, :block], returned[:, block:]], axis=2)
        returned = returned.reshape(rows, width).astype(BF16)
        mixture = dot(r.mix_hi[...].reshape(nk * seqs, rows), returned) + dot(
            r.mix_lo[...].reshape(nk * seqs, rows), returned
        )
        r.mix_out[...] = mixture.reshape(nk, seqs, width).astype(BF16)
    for q in others:
        send(r.mix_out.at[q], r.mix_in.at[q], r.mix_send.at[0], r.mix_recv.at[0], back_plane(q))
    with scope("final"):
        total = mixture[0:seqs]
        settle(r.mix_in.at[pl.ds(1, nk - 1)], r.mix_recv.at[0])
        for q in range(1, nk):
            total = total + r.mix_in[q].astype(F32)
        r.layer_out[...] = (r.resid[0, 0:seqs, :].astype(F32) + total).astype(BF16)
    with scope("drain"):
        settle(r.part_in.at[pl.ds(1, ny - 1)], r.part_send.at[0])
        settle(r.info_in.at[pl.ds(1, nk - 1)], r.info_send.at[0])
        settle(r.resid.at[pl.ds(1, nk - 1), pl.ds(0, seqs)], r.res_send.at[0])
        settle(r.z_in.at[pl.ds(1, nz - 1)], r.z_send.at[0])
        settle(r.y_in.at[pl.ds(1, ny - 1)], r.y_send.at[0])
        settle(r.share_in.at[pl.ds(1, ny - 1)], r.share_send.at[0])
        settle(r.back_in.at[pl.ds(1, nz - 1)], r.back_send.at[0])
        settle(r.mix_in.at[pl.ds(1, nk - 1)], r.mix_send.at[0])


def run_layer(sizes, *operands):
    nz, nk, ny, seqs, width = sizes
    args = dict(zip(INPUTS, operands, strict=True))
    rows = nz * SLOTS * nk
    message = (2 * SLOTS * nk, width // 2)
    hidden = args["gate"].shape[2]
    wide = args["recept"].shape[1]
    low = args["decay_down"].shape[0]
    state = args["state"].shape
    heads = state[1]
    dma = pltpu.SemaphoreType.DMA
    scratch = dict(
        tokens_vm=pltpu.VMEM((seqs, ny * width), BF16),
        qkv_vm=pltpu.VMEM((ny * width, 3 * wide), BF16),
        low_vm=pltpu.VMEM((2 * low, ny * width), BF16),
        up_vm=pltpu.VMEM((2 * low, 2 * wide), BF16),
        base_vm=pltpu.VMEM((1, wide), F32),
        rate_vm=pltpu.VMEM((1, wide), F32),
        gain_vm=pltpu.VMEM((1, wide), F32),
        routes_vm=pltpu.VMEM(args["routes"].shape, I32),
        weights_vm=pltpu.VMEM(args["weights"].shape, F32),
        vec_vm=pltpu.VMEM((3 * heads, seqs, wide), F32),
        col_vm=pltpu.VMEM((2, seqs, wide), F32),
        out_vm=pltpu.VMEM((wide, ny * width), BF16),
        gu_vm=pltpu.VMEM((ny * width, 2 * hidden), BF16),
        down_vm=pltpu.VMEM((hidden, ny * width), BF16),
        info_out=pltpu.VMEM((nk, 2 * nz, LANES), F32),
        info_in=pltpu.VMEM((nk, 2 * nz, LANES), F32),
        part_out=pltpu.VMEM((ny, seqs, width), BF16),
        part_in=pltpu.VMEM((ny, seqs, width), BF16),
        resid=pltpu.VMEM((nk, LANES, width), BF16),
        pick=pltpu.VMEM((rows, nk * LANES), BF16),
        mix_hi=pltpu.VMEM((nk, seqs, rows), BF16),
        mix_lo=pltpu.VMEM((nk, seqs, rows), BF16),
        z_out=pltpu.VMEM((nz, *message), BF16),
        z_in=pltpu.VMEM((nz, *message), BF16),
        y_in=pltpu.VMEM((ny, nz, *message), BF16),
        share_out=pltpu.VMEM((ny, nz, *message), BF16),
        share_in=pltpu.VMEM((ny, nz, *message), BF16),
        back_out=pltpu.VMEM((nz, *message), BF16),
        back_in=pltpu.VMEM((nz, *message), BF16),
        mix_out=pltpu.VMEM((nk, seqs, width), BF16),
        mix_in=pltpu.VMEM((nk, seqs, width), BF16),
        load_sem=dma((9 + seqs // 8,)),
    )
    waits = len(plane_groups(nz))
    for name, count in dict(
        info=1, part=1, res=1, z=nz, y=waits, share=waits, back=1, mix=1
    ).items():
        scratch[name + "_send"] = dma((1,))
        scratch[name + "_recv"] = dma((count,))
    hbm = pl.BlockSpec(memory_space=pltpu.HBM)
    vmem = pl.BlockSpec(memory_space=pltpu.VMEM)
    names = INPUTS + ["layer_out", "new_state"] + list(scratch)
    outs = ((seqs, width), BF16), (state, F32)
    results = pl.pallas_call(
        functools.partial(layer_kernel, sizes, names),
        out_shape=tuple(pltpu.VMEM(*out) for out in outs),
        in_specs=[hbm] * len(INPUTS),
        out_specs=(vmem, vmem),
        scratch_shapes=list(scratch.values()),
        compiler_params=pltpu.CompilerParams(
            collective_id=0, has_side_effects=True, vmem_limit_bytes=60 * 1024 * 1024
        ),
        name="layer",
    )(*operands)
    return pl.pallas_call(
        store_kernel,
        out_shape=tuple(jax.ShapeDtypeStruct(*out) for out in outs),
        in_specs=[vmem, vmem],
        out_specs=(hbm, hbm),
        scratch_shapes=[dma((PIECES + 1,))],
        compiler_params=pltpu.CompilerParams(vmem_limit_bytes=1024 * 1024),
        name="store",
    )(*results)


def store_kernel(layer_vm, state_vm, layer_ref, state_ref, sems):
    size = state_vm.shape[0] // PIECES
    copies = [pltpu.make_async_copy(layer_vm, layer_ref, sems.at[PIECES])]
    for i in range(PIECES):
        at = pl.ds(i * size, size)
        copies.append(pltpu.make_async_copy(state_vm.at[at], state_ref.at[at], sems.at[i]))
    for copy in copies:
        copy.start()
    for copy in copies:
        copy.wait()


def local(
    tokens,
    head_state,
    recept_weight,
    key_weight,
    value_weight,
    decay_down_factor,
    decay_up_factor,
    decay_base,
    rate_down_factor,
    rate_up_factor,
    rate_base,
    head_gain,
    out_weight,
    route_experts,
    route_weights,
    expert_gate,
    expert_up,
    expert_down,
):
    ny = lax.axis_size("tp")
    nz = lax.axis_size("ep") // PLANE
    seqs, model = tokens.shape

    return run_layer(
        (nz, PLANE, ny, seqs, model // ny),
        tokens,
        head_state,
        recept_weight,
        key_weight,
        value_weight,
        decay_down_factor.T,
        decay_up_factor,
        decay_base[None],
        rate_down_factor.T,
        rate_up_factor,
        rate_base[None],
        head_gain[None],
        out_weight,
        route_experts.T,
        route_weights.T,
        expert_gate,
        expert_up,
        expert_down,
    )


def solution(mesh):
    in_specs = (
        P("ep", None),
        P("ep", "tp", None, None),
        P(None, "tp"),
        P(None, "tp"),
        P(None, "tp"),
        P(),
        P(None, "tp"),
        P("tp"),
        P(),
        P(None, "tp"),
        P("tp"),
        P("tp"),
        P("tp", None),
        P("ep", None),
        P("ep", None),
        P("ep", None, "tp"),
        P("ep", None, "tp"),
        P("ep", "tp", None),
    )
    out_specs = (P("ep", "tp"), P("ep", "tp", None, None))
    return jax.shard_map(local, mesh=mesh, in_specs=in_specs, out_specs=out_specs, check_vma=False)
```
